128 devices in a mesh: rep: 2 (over z_hi), fs: 32 (over z_lo, y, x), tp: 2 (over core).
Axes of the slice: x: 4, y: 4, z: 4 (z_hi: 2, z_lo: 2; z = z_hi * 2 + z_lo), core: 2. Of those that a mesh axis runs over, the one named last changes fastest.
Arguments:
- stream: bfloat16 [64, 512, 2048], P(('rep', 'fs'), None, 'tp'), may hold values from -60 to 60
- pre_gain_mix: float32 [2048], P('tp'), may hold values from 0.1 to 1.9
- value_weight: bfloat16 [2048, 2048], P('fs', 'tp'), may hold values from -0.125 to 0.125
- gate_weight: bfloat16 [2048, 2048], P('fs', 'tp'), may hold values from -0.125 to 0.125
- mix_kernel: bfloat16 [31, 2048], P(None, 'tp'), may hold values from -2 to 2
- mix_bias: float32 [2048], P('tp'), may hold values from -2 to 8
- chan_gain: float32 [2048], P('tp'), may hold values from 0.1 to 1.9
- proj_weight: bfloat16 [2048, 2048], P('fs', 'tp'), may hold values from -2 to 2
- post_gain_mix: float32 [2048], P('tp'), may hold values from 0.1 to 1.9
- pre_gain_ffn: float32 [2048], P('tp'), may hold values from 0.1 to 1.9
- up_gate_weight: bfloat16 [2048, 2816], P('fs', 'tp'), may hold values from -0.125 to 0.125
- up_value_weight: bfloat16 [2048, 2816], P('fs', 'tp'), may hold values from -0.125 to 0.125
- gate_kernel: bfloat16 [3, 2816], P(None, 'tp'), may hold values from -2.5 to 2.5
- value_kernel: bfloat16 [3, 2816], P(None, 'tp'), may hold values from -2.5 to 2.5
- down_weight: bfloat16 [2048, 2816], P('fs', 'tp'), may hold values from -2 to 2
- post_gain_ffn: float32 [2048], P('tp'), may hold values from 0.1 to 1.9
Outputs:
- out_stream: bfloat16 [64, 512, 2048], P(('rep', 'fs'), None, 'tp')
The draws below stay inside these ranges and needn't reach their ends.
All inputs are finite; a program needn't handle non-finite values.
Results may differ from the reference program's by a relative error of at most 0.014.
Values may be sent and summed in bfloat16 or wider, within the bound.
A program may use at most 128 MiB of HBM per device.

```python
import math
import jax
import jax.numpy as jnp
from jax import lax

D = 2048
F = 2816
KW = 31
FW = 3
LEN = 512
SEQS = 64
N_TP = 2


def channel_ramp(count, top):
    return jnp.exp(jnp.linspace(0.0, math.log(top), count)).astype(jnp.float32)


def draw_stream(key, part):
    key = jax.random.fold_in(key, 11)
    values = jnp.clip(jax.random.normal(key, (SEQS, LEN, D), jnp.float32), -4.0, 4.0)
    return (values * channel_ramp(D, 3.0)).astype(jnp.bfloat16)


def draw_mix_kernel(key, part):
    key = jax.random.fold_in(key, 23)
    values = jnp.clip(jax.random.normal(key, (KW, D), jnp.float32), -3.0, 3.0)
    return (values * KW ** (-0.5) * channel_ramp(D, 3.0)).astype(jnp.bfloat16)


def draw_mix_bias(key, part):
    key = jax.random.fold_in(key, 31)
    rough = jnp.clip(jax.random.normal(key, (D,), jnp.float32), -3.0, 3.0) * 0.5
    return (rough + jnp.linspace(0.0, 3.0, D)).astype(jnp.float32)


def draw_proj_weight(key, part):
    key = jax.random.fold_in(key, 37)
    values = jnp.clip(jax.random.normal(key, (D, D), jnp.float32), -3.0, 3.0)
    return (values * D ** (-0.5) * channel_ramp(D, 3.0)[:, None]).astype(jnp.bfloat16)


def draw_down_weight(key, part):
    key = jax.random.fold_in(key, 53)
    values = jnp.clip(jax.random.normal(key, (D, F), jnp.float32), -3.0, 3.0)
    return (values * F ** (-0.5) * channel_ramp(D, 3.0)[:, None]).astype(jnp.bfloat16)


def block_levels(own_key, dims, pieces, low, high):
    def one(dim, blocks):
        heights = jax.random.uniform(jax.random.fold_in(jax.random.fold_in(own_key, 6), dim), (blocks,), jnp.float32, low / len(pieces), high / len(pieces))
        return jnp.repeat(jnp.exp(heights), dims[dim] // blocks).reshape((-1,) + (1,) * (len(dims) - dim - 1))

    factor_of = one(*pieces[0])
    for cut in pieces[1:]:
        factor_of = factor_of * one(*cut)
    return factor_of


def normal_values(own_key, dims, scale, most, cuts=(), kind=jnp.bfloat16):
    result = jax.random.normal(own_key, dims, jnp.float32) * scale
    if len(cuts) > 0:
        result = block_levels(own_key, dims, cuts, -0.22, 0.18) * result
    return jnp.clip(result, min=-most, max=most).astype(kind)


def setup_inputs(seed: int = 0) -> dict:
    seeds = jax.random.split(jax.random.key(seed), 17)
    stream = draw_stream(jax.random.fold_in(seeds[16], 71), 0)
    pre_gain_mix = jnp.clip(1.0 + 0.18 * jax.random.normal(seeds[1], (D,), jnp.float32), 0.1, 1.9)
    value_weight = normal_values(seeds[2], (D, D), D ** -0.5, 0.125, ((0, 32), (1, 2)))
    gate_weight = normal_values(seeds[3], (D, D), D ** -0.5, 0.125, ((0, 32), (1, 2)))
    mix_kernel = draw_mix_kernel(jax.random.fold_in(seeds[16], 71), 0)
    mix_bias = draw_mix_bias(jax.random.fold_in(seeds[16], 71), 0)
    chan_gain = jnp.clip(1.0 + 0.18 * jax.random.normal(seeds[6], (D,), jnp.float32), 0.1, 1.9)
    proj_weight = draw_proj_weight(jax.random.fold_in(seeds[16], 71), 0)
    post_gain_mix = jnp.clip(1.0 + 0.18 * jax.random.normal(seeds[8], (D,), jnp.float32), 0.1, 1.9)
    pre_gain_ffn = jnp.clip(1.0 + 0.18 * jax.random.normal(seeds[9], (D,), jnp.float32), 0.1, 1.9)
    up_gate_weight = normal_values(seeds[10], (D, F), D ** -0.5, 0.125, ((0, 32), (1, 2)))
    up_value_weight = normal_values(seeds[11], (D, F), D ** -0.5, 0.125, ((0, 32), (1, 2)))
    gate_kernel = normal_values(seeds[12], (FW, F), 0.577, 2.5, ((1, 2),))
    value_kernel = normal_values(seeds[13], (FW, F), 0.577, 2.5, ((1, 2),))
    down_weight = draw_down_weight(jax.random.fold_in(seeds[16], 71), 0)
    post_gain_ffn = jnp.clip(1.0 + 0.18 * jax.random.normal(seeds[15], (D,), jnp.float32), 0.1, 1.9)
    return dict(stream=stream, pre_gain_mix=pre_gain_mix, value_weight=value_weight, gate_weight=gate_weight, mix_kernel=mix_kernel, mix_bias=mix_bias, chan_gain=chan_gain, proj_weight=proj_weight, post_gain_mix=post_gain_mix, pre_gain_ffn=pre_gain_ffn, up_gate_weight=up_gate_weight, up_value_weight=up_value_weight, gate_kernel=gate_kernel, value_kernel=value_kernel, down_weight=down_weight, post_gain_ffn=post_gain_ffn)


EPS = 1e-06

def rms_apply(values, gain_vector):
    values32 = values.astype(jnp.float32)
    inverse_rms = lax.rsqrt(lax.optimization_barrier(jnp.mean(values32 * values32, axis=-1, keepdims=True)) + EPS)
    return values32 * inverse_rms * gain_vector

def causal_conv(sequence, kernel):
    taps = kernel.shape[0]
    length = sequence.shape[0]
    padded = jnp.pad(sequence.astype(jnp.float32), ((taps - 1, 0), (0, 0)))
    running = jnp.zeros(sequence.shape, jnp.float32)
    for offset in range(taps):
        running = running + kernel[offset].astype(jnp.float32) * padded[offset:offset + length]
    return running

def split_product(activated, weight_rows):
    block_width = activated.shape[1] // N_TP
    running = jnp.zeros((activated.shape[0], weight_rows.shape[0]), jnp.float32)
    for block_index in range(N_TP):
        lower = block_index * block_width
        partial_sum = lax.dot_general(activated[:, lower:lower + block_width], weight_rows[:, lower:lower + block_width], (((1,), (1,)), ((), ())), preferred_element_type=jnp.float32)
        rounded = lax.optimization_barrier(partial_sum.astype(jnp.bfloat16))
        running = running + rounded.astype(jnp.float32)
    return running

def reference(stream, pre_gain_mix, value_weight, gate_weight, mix_kernel, mix_bias, chan_gain, proj_weight, post_gain_mix, pre_gain_ffn, up_gate_weight, up_value_weight, gate_kernel, value_kernel, down_weight, post_gain_ffn):

    def one_sequence(sequence):
        normed = rms_apply(sequence, pre_gain_mix).astype(jnp.bfloat16)
        value_part = jnp.dot(normed, value_weight, preferred_element_type=jnp.float32)
        gate_part = jnp.dot(normed, gate_weight, preferred_element_type=jnp.float32)
        glu = (value_part * jax.nn.sigmoid(gate_part)).astype(jnp.bfloat16)
        convolved = causal_conv(glu, mix_kernel) + mix_bias
        chan_mean = lax.optimization_barrier(jnp.mean(convolved, axis=-1, keepdims=True))
        centred = convolved - chan_mean
        chan_var = lax.optimization_barrier(jnp.mean(centred * centred, axis=-1, keepdims=True))
        activated = jax.nn.silu(centred * lax.rsqrt(chan_var + EPS) * chan_gain).astype(jnp.bfloat16)
        mixed = split_product(activated, proj_weight).astype(jnp.bfloat16)
        middle = (sequence.astype(jnp.float32) + rms_apply(mixed, post_gain_mix)).astype(jnp.bfloat16)
        normed_ffn = rms_apply(middle, pre_gain_ffn).astype(jnp.bfloat16)
        up_gate = jnp.dot(normed_ffn, up_gate_weight, preferred_element_type=jnp.float32).astype(jnp.bfloat16)
        up_value = jnp.dot(normed_ffn, up_value_weight, preferred_element_type=jnp.float32).astype(jnp.bfloat16)
        hidden = (jax.nn.silu(causal_conv(up_gate, gate_kernel)) * causal_conv(up_value, value_kernel)).astype(jnp.bfloat16)
        ffn_out = split_product(hidden, down_weight).astype(jnp.bfloat16)
        return (middle.astype(jnp.float32) + rms_apply(ffn_out, post_gain_ffn)).astype(jnp.bfloat16)
    return lax.map(one_sequence, stream)
```

```python
import functools

import jax
import jax.numpy as jnp
from jax import lax
from jax.experimental import pallas as pl
from jax.experimental.pallas import tpu as pltpu
from jax.sharding import PartitionSpec as P

EPS = 1e-06
MESH = pl.DeviceIdType.MESH
F32, BF16 = jnp.float32, jnp.bfloat16

VARIANTS = ((0, 1), (0, -1), (1, 1), (1, -1))
ZSIGN = (1, -1, -1, 1)

class Place:
    def __init__(s):
        fs = lax.axis_index("fs"); zh = lax.axis_index("rep")
        s.core = lax.axis_index("tp")
        s.x = fs % 4; s.y = (fs // 4) % 4; s.zl = fs // 16
        s.z = zh * 2 + s.zl
    def dev(s, dx=0, dy=0, dz=0):
        x = (s.x + dx + 4) % 4; y = (s.y + dy + 4) % 4; z = (s.z + dz + 4) % 4
        return (z // 2, (z % 2) * 16 + y * 4 + x, s.core)
    def partner(s):
        return (lax.axis_index("rep"), lax.axis_index("fs"), 1 - s.core)

class Unit:
    def __init__(s, place, buf, m, split, cols, lo, ssem, rsem, u):
        s.p, s.buf, s.m = place, buf, m
        s.c1 = pl.ds(lo, split); s.c2 = pl.ds(lo + split, cols - split)
        s.ssem, s.rsem, s.u = ssem, rsem, u
        s.sent = []
    def reg(s, q, kind, content, da, db):
        p = s.p; first = VARIANTS[q][0]
        rows = pl.ds(16 * q, 16)
        cols = s.c1 if kind == 1 else s.c2
        zi = slice(None) if content is None else content
        if da is None:
            b = (( p.y if first == 0 else p.x) + db + 4) % 4
            return s.buf.at[s.m, zi, b, :, rows, cols] if first == 0 else s.buf.at[s.m, zi, :, b, rows, cols]
        a = ((p.x if first == 0 else p.y) + da + 4) % 4
        b = ((p.y if first == 0 else p.x) + db + 4) % 4
        y, x = (b, a) if first == 0 else (a, b)
        return s.buf.at[s.m, zi, y, x, rows, cols]
    def to(s, q, da=0, db=0, dz=0):
        first = VARIANTS[q][0]
        return s.p.dev(da, db, dz) if first == 0 else s.p.dev(db, da, dz)
    def copy(s, q, n, region, dev):
        return pltpu.make_async_remote_copy(src_ref=region, dst_ref=region, send_sem=s.ssem.at[s.u, q, n],
            recv_sem=s.rsem.at[s.u, q, n], device_id=dev, device_id_type=MESH)
    def send(s, q, n, region, dev):
        c = s.copy(q, n, region, dev); c.start(); s.sent.append((q, n, region))
    def wait(s, q, n, region):
        s.copy(q, n, region, s.p.dev()).wait_recv()
    def drain(s):
        for q, n, region in s.sent:
            s.copy(q, n, region, s.p.dev()).wait_send()
    def stage(s, k, q):
        mine, other = s.p.zl, 1 - s.p.zl
        f = VARIANTS[q][1]; z = ZSIGN[q]
        near, far = ((0, 1) if f > 0 else (1, 0))
        R, S, W, T = s.reg, s.send, s.wait, s.to
        if k == 0:
            S(q, 0, R(q, 1, mine, 0, 0), T(q, 1)); S(q, 1, R(q, 1, mine, 0, 0), T(q, -1))
            S(q, 10, R(q, 2, mine, 0, 0), T(q, dz=z))
        elif k == 1:
            W(q, near, R(q, 1, mine, -f, 0)); S(q, 2, R(q, 1, mine, -f, 0), T(q, f))
            W(q, 10, R(q, 2, other, 0, 0))
            S(q, 11, R(q, 2, None, 0, 0), T(q, 1)); S(q, 12, R(q, 2, None, 0, 0), T(q, -1))
        elif k == 2:
            W(q, far, R(q, 1, mine, f, 0)); W(q, 2, R(q, 1, mine, 2, 0))
            S(q, 3, R(q, 1, mine, None, 0), T(q, 0, 1)); S(q, 4, R(q, 1, mine, None, 0), T(q, 0, -1))
            S(q, 6, R(q, 1, mine, None, 0), T(q, dz=z))
            W(q, 11 + near, R(q, 2, None, -f, 0)); S(q, 13, R(q, 2, None, -f, 0), T(q, f))
        elif k == 3:
            W(q, 3 + near, R(q, 1, mine, None, -f)); S(q, 5, R(q, 1, mine, None, -f), T(q, 0, f))
            S(q, 7, R(q, 1, mine, None, -f), T(q, dz=z))
            W(q, 3 + far, R(q, 1, mine, None, f)); S(q, 8, R(q, 1, mine, None, f), T(q, dz=z))
            W(q, 11 + far, R(q, 2, None, f, 0)); W(q, 13, R(q, 2, None, 2, 0))
            S(q, 14, R(q, 2, None, None, 0), T(q, 0, 1)); S(q, 15, R(q, 2, None, None, 0), T(q, 0, -1))
        elif k == 4:
            W(q, 5, R(q, 1, mine, None, 2)); S(q, 9, R(q, 1, mine, None, 2), T(q, dz=z))
            W(q, 14 + near, R(q, 2, None, None, -f)); S(q, 16, R(q, 2, None, None, -f), T(q, 0, f))
        elif k == 5:
            W(q, 14 + far, R(q, 2, None, None, f)); W(q, 16, R(q, 2, None, None, 2))
            W(q, 6, R(q, 1, other, None, 0)); W(q, 7, R(q, 1, other, None, -f))
            W(q, 8, R(q, 1, other, None, f)); W(q, 9, R(q, 1, other, None, 2))

def tick(units, t, order=(5, 4, 3, 2, 1, 0)):
    for k in order:
        if 0 <= t - k < len(units):
            for q in range(4):
                units[t - k].stage(k, q)

def barrier(p):
    sem = pltpu.get_barrier_semaphore()
    ds = [p.dev(1), p.dev(-1), p.dev(0, 1), p.dev(0, -1), p.dev(0, 0, 1), p.dev(0, 0, -1), p.partner()]
    for d in ds:
        pl.semaphore_signal(sem, inc=1, device_id=d, device_id_type=MESH)
    pl.semaphore_wait(sem, len(ds))


UNITS = ((0, 0, 1024, 640), (1, 0, 1024, 640), (2, 0, 1024, 640), (3, 0, 1408, 896), (4, 0, 1408, 896), (5, 0, 1408, 896))
ROWS = 512
HALF = 1024
HID = 1408


def norm_rows(a, b, width):
    total = jnp.sum(a * a, axis=1, keepdims=True) + jnp.sum(b * b, axis=1, keepdims=True)
    return lax.rsqrt(total * (1.0 / width) + EPS)


def kernel(
    stream_in, pre_mix_in, value_in, gate_in, taps_in, bias_in, chan_in, proj_in, post_mix_in, pre_ffn_in,
    up_gate_in, up_value_in, gate_taps_in, value_taps_in, down_in, post_ffn_in,
    out,
    wm, wf, xs, xn, val, glu, act, pm, rm, pf, rf, mid, upg, upv, hid, st, gains, taps_b, taps, gtaps_b, vtaps_b, outb,
    ssem, rsem, lsem, psend, precv, osem,
):
    p = Place()
    core = p.core
    partner = p.partner()

    def trade(n, src, dst):
        return pltpu.make_async_remote_copy(
            src_ref=src, dst_ref=dst, send_sem=psend.at[n], recv_sem=precv.at[n], device_id=partner, device_id_type=MESH
        )

    weights = (value_in, gate_in, proj_in, up_gate_in, up_value_in, down_in)
    loads = [
        pltpu.make_async_copy(w, (wm.at[i] if i < 3 else wf.at[i - 3]).at[p.zl, p.y, p.x], lsem.at[i])
        for i, w in enumerate(weights)
    ]
    vectors = (pre_mix_in, post_mix_in, pre_ffn_in, post_ffn_in, bias_in, chan_in)
    small = [pltpu.make_async_copy(stream_in.at[0], xs.at[core], lsem.at[6])]
    small += [pltpu.make_async_copy(v, gains.at[core, i], lsem.at[7 + i]) for i, v in enumerate(vectors)]
    small += [
        pltpu.make_async_copy(taps_in, taps_b, lsem.at[13]),
        pltpu.make_async_copy(gate_taps_in, gtaps_b, lsem.at[14]),
        pltpu.make_async_copy(value_taps_in, vtaps_b, lsem.at[15]),
    ]
    for c in loads + small:
        c.start()
    barrier(p)
    for c in loads:
        c.wait()
    units = [
        Unit(p, wm if m < 3 else wf, m % 3, split, cols, lo, ssem, rsem, u)
        for u, (m, lo, cols, split) in enumerate(UNITS)
    ]
    step = functools.partial(tick, units)
    step(0)
    for c in small:
        c.wait()
    swap_x = trade(0, xs.at[core], xs.at[core])
    swap_g = trade(1, gains.at[core], gains.at[core])
    swap_x.start()
    swap_g.start()
    step(1)
    trade(0, xs.at[1 - core], xs.at[1 - core]).wait_recv()
    trade(1, gains.at[1 - core], gains.at[1 - core]).wait_recv()

    def first_norm(i, _):
        r = pl.ds(pl.multiple_of(i * 16, 16), 16)
        a, b = xs[0, r, :].astype(F32), xs[1, r, :].astype(F32)
        inv = norm_rows(a, b, 2 * HALF)
        xn[0, r, :] = (a * inv * gains[0, 0]).astype(BF16)
        xn[1, r, :] = (b * inv * gains[1, 0]).astype(BF16)
        return 0

    step(2)
    lax.fori_loop(0, ROWS // 16, first_norm, 0)
    taps[0:31, :] = taps_b[...].astype(F32)
    glu[0:32, :] = jnp.zeros((32, HALF), F32)
    upg[0:8, :] = jnp.zeros((8, HID), F32)
    upv[0:8, :] = jnp.zeros((8, HID), F32)

    def product(buf, m, c):
        w0 = buf[m, 0, :, :, :, c].reshape(HALF, c.size)
        w1 = buf[m, 1, :, :, :, c].reshape(HALF, c.size)
        return jnp.dot(xn[0], w0, preferred_element_type=F32) + jnp.dot(xn[1], w1, preferred_element_type=F32)

    def blocks(width, body):
        def one(i, _):
            body(pl.ds(pl.multiple_of(i * 256, 256), 256))
            return 0

        lax.fori_loop(0, width // 256, one, 0)
        if width % 256:
            body(pl.ds(width // 256 * 256, width % 256))

    step(3)
    step(4)
    step(5)

    def value_block(c):
        val[:, c] = product(wm, 0, c)

    blocks(HALF, value_block)
    step(6)

    def gate_block(c):
        g = product(wm, 1, c)
        glu[32 : 32 + ROWS, c] = (val[:, c] * jax.nn.sigmoid(g)).astype(BF16).astype(F32)

    blocks(HALF, gate_block)

    def conv_block(i, _):
        c = pl.ds(pl.multiple_of((i % 8) * 128, 128), 128)
        t = pl.multiple_of((i // 8) * 64, 64)
        g = glu[pl.ds(t, 96), c]
        total = jnp.broadcast_to(gains[core, 4, :, c], (64, 128))
        for k in range(8):
            part = None
            rows = 72 if k else 64
            for j in range(31):
                if (2 + j) % 8 == k:
                    at = (2 + j) // 8 * 8
                    term = taps[j : j + 1, c] * g[at : at + rows]
                    part = term if part is None else part + term
            total = total + part[k : k + 64]
        val[pl.ds(t, 64), c] = total
        return 0

    lax.fori_loop(0, 64, conv_block, 0)

    def stats_block(i, _):
        r = pl.ds(pl.multiple_of(i * 32, 32), 32)
        v = val[r, :]
        mean = jnp.sum(v, axis=1, keepdims=True) * (1.0 / HALF)
        d = v - mean
        st[core, 0, r, :] = jnp.broadcast_to(mean, (32, 128))
        st[core, 1, r, :] = jnp.broadcast_to(jnp.sum(d * d, axis=1, keepdims=True), (32, 128))
        return 0

    lax.fori_loop(0, ROWS // 32, stats_block, 0)
    swap_s = trade(2, st.at[core], st.at[core])
    swap_s.start()
    step(7)
    trade(2, st.at[1 - core], st.at[1 - core]).wait_recv()

    def act_block(i, _):
        r = pl.ds(pl.multiple_of(i * 32, 32), 32)
        m0, m1 = st[0, 0, r, :][:, :1], st[1, 0, r, :][:, :1]
        gap = m0 - m1
        var = (st[0, 1, r, :][:, :1] + st[1, 1, r, :][:, :1] + gap * gap * (HALF / 2)) * (0.5 / HALF)
        h = (val[r, :] - (m0 + m1) * 0.5) * lax.rsqrt(var + EPS) * gains[core, 5]
        act[r, :] = jax.nn.silu(h).astype(BF16)
        return 0

    lax.fori_loop(0, ROWS // 32, act_block, 0)

    def rows_product(lhs, buf, mine, theirs, base):
        def region(ref, i):
            return ref.at[i // 4, :, pl.ds(pl.multiple_of((i % 4) * 256, 256), 256)]

        def send(i):
            trade(base + i, region(mine, i), region(theirs, i)).start()

        def one(i, _):
            w = buf[2, i // 4, i % 4].reshape(256, lhs.shape[1])
            part = lax.dot_general(lhs[...], w, (((1,), (1,)), ((), ())), preferred_element_type=F32)
            mine[i // 4, :, pl.ds(pl.multiple_of((i % 4) * 256, 256), 256)] = part.astype(BF16)

            @pl.when(i > 0)
            def _():
                send(i - 1)

            return 0

        lax.fori_loop(0, 8, one, 0)
        send(7)

        def arrive(i, _):
            trade(base + i, region(theirs, i), region(theirs, i)).wait_recv()
            return 0

        def leave(i, _):
            trade(base + i, region(mine, i), region(theirs, i)).wait_send()
            return 0

        return lambda: lax.fori_loop(0, 8, arrive, 0), lambda: lax.fori_loop(0, 8, leave, 0)

    mix_arrive, mix_leave = rows_product(act, wm, pm, rm, 3)
    step(8)
    mix_arrive()

    def middle_block(i, _):
        r = pl.ds(pl.multiple_of(i * 16, 16), 16)
        a = (pm[0, r, :].astype(F32) + rm[0, r, :].astype(F32)).astype(BF16).astype(F32)
        b = (pm[1, r, :].astype(F32) + rm[1, r, :].astype(F32)).astype(BF16).astype(F32)
        inv = norm_rows(a, b, 2 * HALF)
        a = (xs[0, r, :].astype(F32) + a * inv * gains[0, 1]).astype(BF16)
        b = (xs[1, r, :].astype(F32) + b * inv * gains[1, 1]).astype(BF16)
        mid[0, r, :] = a
        mid[1, r, :] = b
        a, b = a.astype(F32), b.astype(F32)
        inv = norm_rows(a, b, 2 * HALF)
        xn[0, r, :] = (a * inv * gains[0, 2]).astype(BF16)
        xn[1, r, :] = (b * inv * gains[1, 2]).astype(BF16)
        return 0

    lax.fori_loop(0, ROWS // 16, middle_block, 0)

    def up_block(dst, m, c):
        dst[8 : 8 + ROWS, c] = product(wf, m, c).astype(BF16).astype(F32)

    blocks(HID, functools.partial(up_block, upg, 0))
    step(9)
    blocks(HID, functools.partial(up_block, upv, 1))

    def hidden_block(i, _):
        c = pl.ds(pl.multiple_of((i // 8) * 128, 128), 128)
        t = pl.multiple_of((i % 8) * 64, 64)
        g, v = upg[pl.ds(t, 72), c], upv[pl.ds(t, 72), c]
        kg, kv = gtaps_b[:, c].astype(F32), vtaps_b[:, c].astype(F32)
        gc = kg[0:1] * g[6:70] + kg[1:2] * g[7:71] + kg[2:3] * g[8:72]
        vc = kv[0:1] * v[6:70] + kv[1:2] * v[7:71] + kv[2:3] * v[8:72]
        hid[pl.ds(t, 64), c] = (jax.nn.silu(gc) * vc).astype(BF16)
        return 0

    lax.fori_loop(0, 8 * (HID // 128), hidden_block, 0)
    step(10)
    ffn_arrive, ffn_leave = rows_product(hid, wf, pf, rf, 11)
    ffn_arrive()

    def out_block(i, _):
        r = pl.ds(pl.multiple_of(i * 16, 16), 16)
        a = (pf[core, r, :].astype(F32) + rf[core, r, :].astype(F32)).astype(BF16).astype(F32)
        b = (pf[1 - core, r, :].astype(F32) + rf[1 - core, r, :].astype(F32)).astype(BF16).astype(F32)
        inv = norm_rows(a, b, 2 * HALF)
        outb[r, :] = (mid[core, r, :].astype(F32) + a * inv * gains[core, 3]).astype(BF16)
        return 0

    stores = []
    for k in range(4):
        lax.fori_loop(8 * k, 8 * k + 8, out_block, 0)
        c = pltpu.make_async_copy(outb.at[pl.ds(128 * k, 128)], out.at[0, pl.ds(128 * k, 128)], osem.at[k])
        c.start()
        stores.append(c)
    swap_x.wait_send()
    swap_g.wait_send()
    swap_s.wait_send()
    mix_leave()
    ffn_leave()
    for u in units:
        u.drain()
    for c in stores:
        c.wait()


def per_device(*args):
    arrays = [a.reshape(1, -1) if a.ndim == 1 else a for a in args]
    sems = pltpu.SemaphoreType.DMA
    return pl.pallas_call(
        kernel,
        out_shape=jax.ShapeDtypeStruct((1, ROWS, HALF), BF16),
        in_specs=[pl.BlockSpec(memory_space=pl.ANY)] * len(arrays),
        out_specs=pl.BlockSpec(memory_space=pl.ANY),
        scratch_shapes=[
            pltpu.VMEM((3, 2, 4, 4, 64, HALF), BF16),
            pltpu.VMEM((3, 2, 4, 4, 64, HID), BF16),
            pltpu.VMEM((2, ROWS, HALF), BF16),
            pltpu.VMEM((2, ROWS, HALF), BF16),
            pltpu.VMEM((ROWS, HALF), F32),
            pltpu.VMEM((32 + ROWS, HALF), F32),
            pltpu.VMEM((ROWS, HALF), BF16),
            pltpu.VMEM((2, ROWS, HALF), BF16),
            pltpu.VMEM((2, ROWS, HALF), BF16),
            pltpu.VMEM((2, ROWS, HALF), BF16),
            pltpu.VMEM((2, ROWS, HALF), BF16),
            pltpu.VMEM((2, ROWS, HALF), BF16),
            pltpu.VMEM((8 + ROWS, HID), F32),
            pltpu.VMEM((8 + ROWS, HID), F32),
            pltpu.VMEM((ROWS, HID), BF16),
            pltpu.VMEM((2, 2, ROWS, 128), F32),
            pltpu.VMEM((2, 6, 1, HALF), F32),
            pltpu.VMEM((31, HALF), BF16),
            pltpu.VMEM((32, HALF), F32),
            pltpu.VMEM((3, HID), BF16),
            pltpu.VMEM((3, HID), BF16),
            pltpu.VMEM((ROWS, HALF), BF16),
            sems((len(UNITS), 4, 17)),
            sems((len(UNITS), 4, 17)),
            sems((16,)),
            sems((19,)),
            sems((19,)),
            sems((4,)),
        ],
        compiler_params=pltpu.CompilerParams(collective_id=0, has_side_effects=True, vmem_limit_bytes=67043328),
    )(*arrays)


def solution(mesh):
    rows = P(("rep", "fs"), None, "tp")
    vector, matrix, taps = P("tp"), P("fs", "tp"), P(None, "tp")
    placed = (
        rows, vector, matrix, matrix, taps, vector, vector, matrix, vector, vector,
        matrix, matrix, taps, taps, matrix, vector,
    )
    return jax.shard_map(per_device, mesh=mesh, in_specs=placed, out_specs=rows, check_vma=False)
```

```python
import functools

import jax
import jax.numpy as jnp
from jax import lax
from jax.experimental import pallas as pl
from jax.experimental.pallas import tpu as pltpu
from jax.sharding import PartitionSpec as P

EPS = 1e-06
MESH = pl.DeviceIdType.MESH
F32, BF16 = jnp.float32, jnp.bfloat16

class Place:
    def __init__(s):
        fs = lax.axis_index("fs"); zh = lax.axis_index("rep")
        s.core = lax.axis_index("tp")
        s.x = fs % 4; s.y = (fs // 4) % 4; s.zl = fs // 16
        s.z = zh * 2 + s.zl
    def dev(s, dx=0, dy=0, dz=0):
        x = (s.x + dx + 4) % 4; y = (s.y + dy + 4) % 4; z = (s.z + dz + 4) % 4
        return (z // 2, (z % 2) * 16 + y * 4 + x, s.core)
    def partner(s):
        return (lax.axis_index("rep"), lax.axis_index("fs"), 1 - s.core)

class Unit:
    WAITS = (6, 7)

    def __init__(s, place, buf, m, lo, cols, split, ssem, rsem, u, base):
        s.p, s.buf, s.m = place, buf, m
        s.c1, s.c2, s.all_columns = pl.ds(lo, split), pl.ds(lo + split, cols - split), pl.ds(lo, cols)
        s.ssem, s.rsem = ssem.at[u], rsem
        s.base = (base, base + (13 if split else 0))

    @staticmethod
    def semaphores(cols, split):
        return (13 if split else 0) + (14 if split < cols else 0)

    def region(s, g, kind, part, content, da, db):
        rows = pl.ds(32 * g + 16 * max(part, 0), 32 if part < 0 else 16)
        cols = s.c1 if kind == 1 else s.c2
        z = slice(None) if content is None else content
        first, second = (s.p.x, s.p.y) if g == 0 else (s.p.y, s.p.x)
        a = slice(None) if da is None else (first + da + 4) % 4
        b = (second + db + 4) % 4
        y, x = (b, a) if g == 0 else (a, b)
        return s.buf.at[s.m, z, y, x, rows, cols]

    def copy(s, n, region, dev):
        return pltpu.make_async_remote_copy(
            src_ref=region, dst_ref=region, send_sem=s.ssem, recv_sem=s.rsem.at[n], device_id=dev, device_id_type=MESH
        )

    def drain(s):
        whole = s.buf.reshape(3, 32, *s.buf.shape[4:]).at[s.m, pl.ds(0, 31), :, s.all_columns]
        s.copy(0, whole, s.p.dev()).wait_send()

    def stage(s, kind, k, g):
        if (s.c1 if kind == 1 else s.c2).size == 0:
            return
        mine, other, R = s.p.zl, 1 - s.p.zl, functools.partial(s.region, g, kind)
        sem = s.base[kind - 1] + g * s.WAITS[kind - 1]
        up = 1 - 2 * g
        signs = ((0, 1), (1, -1))

        def send(n, region, da=0, db=0, dz=0):
            s.copy(sem + n, region, s.p.dev(da, db, dz) if g == 0 else s.p.dev(db, da, dz)).start()

        def to_z(region):
            s.copy(s.base[0] + 12, region, s.p.dev(0, 0, up)).start()

        def wait(n, region):
            s.copy(sem + n, region, s.p.dev()).wait_recv()

        if (kind, k) == (1, 0):
            for i, d in signs:
                send(i, R(-1, mine, 0, 0), d)
        elif (kind, k) == (1, 1):
            for i, d in signs:
                wait(i, R(-1, mine, -d, 0))
                send(2, R(i, mine, -d, 0), d)
        elif (kind, k) == (1, 2):
            wait(2, R(-1, mine, 2, 0))
            for i, d in signs:
                send(3 + i, R(-1, mine, None, 0), 0, d)
            to_z(R(-1, mine, None, 0))
        elif (kind, k) == (1, 3):
            for i, d in signs:
                wait(3 + i, R(-1, mine, None, -d))
                send(5, R(i, mine, None, -d), 0, d)
                to_z(R(-1, mine, None, -d))
        elif (kind, k) == (1, 4):
            wait(5, R(-1, mine, None, 2))
            to_z(R(-1, mine, None, 2))
        elif (kind, k) == (1, 5):
            if g == 0:
                wait(12, s.buf.at[s.m, other, :, :, :, s.c1])
        elif (kind, k) == (2, 0):
            send(0, R(-1, mine, 0, 0), 0, 0, up)
        elif (kind, k) == (2, 1):
            wait(0, R(-1, other, 0, 0))
            for i, d in signs:
                send(1 + i, R(-1, None, 0, 0), d)
        elif (kind, k) == (2, 2):
            for i, d in signs:
                wait(1 + i, R(-1, None, -d, 0))
                send(3, R(i, None, -d, 0), d)
        elif (kind, k) == (2, 3):
            wait(3, R(-1, None, 2, 0))
            for i, d in signs:
                send(4 + i, R(-1, None, None, 0), 0, d)
        elif (kind, k) == (2, 4):
            for i, d in signs:
                wait(4 + i, R(-1, None, None, -d))
                send(6, R(i, None, None, -d), 0, d)
        elif (kind, k) == (2, 5):
            wait(6, R(-1, None, None, 2))


def barrier(p):
    sem = pltpu.get_barrier_semaphore()
    ds = [p.dev(1), p.dev(-1), p.dev(0, 1), p.dev(0, -1), p.dev(0, 0, 1), p.dev(0, 0, -1), p.partner()]
    for d in ds:
        pl.semaphore_signal(sem, inc=1, device_id=d, device_id_type=MESH)
    pl.semaphore_wait(sem, len(ds))


UNITS = (
    (0, pl.ds(0, 2), 0, 1024, 512),
    (0, 2, 0, 1024, 896),
    (1, pl.ds(0, 2), 0, 768, 768),
    (1, pl.ds(0, 2), 768, 640, 256),
    (1, 2, 0, 896, 0),
    (1, 2, 896, 512, 384),
)
DOWN = (0, 896, 1408)
SCHEDULE = (
    ("u", 0, 1, 0), ("u", 0, 2, 0), ("start",), ("u", 1, 1, 0), ("u", 1, 2, 0), ("u", 2, 1, 0), ("u", 3, 2, 0),
    ("u", 3, 1, 0), ("u", 4, 2, 0), ("u", 5, 2, 0), ("u", 5, 1, 0), ("u", 0, 1, 1), ("u", 0, 2, 1), ("norm",),
    ("u", 0, 1, 2), ("u", 0, 2, 2), ("u", 1, 1, 1), ("u", 1, 2, 1), ("u", 0, 1, 3), ("u", 0, 2, 3), ("u", 1, 1, 2),
    ("u", 1, 2, 2), ("u", 2, 1, 1), ("u", 0, 1, 4), ("u", 0, 2, 4), ("u", 1, 1, 3), ("u", 1, 2, 3), ("u", 2, 1, 2),
    ("u", 3, 2, 1), ("u", 3, 1, 1), ("u", 0, 1, 5), ("u", 0, 2, 5), ("glu", 0), ("glu", 1), ("u", 1, 1, 4), ("glu", 2),
    ("u", 1, 2, 4), ("glu", 3), ("conv", 0), ("conv", 1), ("conv", 2), ("conv", 3), ("u", 2, 1, 3), ("stats",),
    ("u", 3, 2, 2), ("u", 3, 1, 2), ("u", 4, 2, 1), ("u", 1, 2, 5), ("act",), ("u", 1, 1, 5), ("u", 2, 1, 4),
    ("u", 3, 2, 3), ("proj", 0), ("u", 3, 1, 3), ("proj", 1), ("u", 4, 2, 2), ("u", 5, 1, 1), ("u", 5, 2, 1),
    ("mid", 0), ("mid", 1), ("u", 3, 2, 4), ("u", 3, 1, 4), ("u", 4, 2, 3), ("u", 5, 1, 2), ("u", 5, 2, 2),
    ("u", 3, 2, 5), ("u", 2, 1, 5), ("up", 0), ("up", 1), ("up", 2), ("hid", 0), ("u", 4, 2, 4), ("hid", 1),
    ("u", 5, 1, 3), ("u", 5, 2, 3), ("u", 3, 1, 5), ("up", 3), ("up", 4), ("up", 5), ("hid", 2), ("u", 4, 2, 5),
    ("hid", 3), ("u", 5, 1, 4), ("u", 5, 2, 4), ("down", 0), ("u", 5, 1, 5), ("u", 5, 2, 5), ("down", 1),
)
ROWS = 512
HALF = 1024
HID = 1408


def norm_rows(a, b, width):
    total = jnp.sum(a * a, axis=1, keepdims=True) + jnp.sum(b * b, axis=1, keepdims=True)
    return lax.rsqrt(total * (1.0 / width) + EPS)


def kernel(
    stream_in, pre_mix_in, value_in, gate_in, taps_in, bias_in, chan_in, proj_in, post_mix_in, pre_ffn_in,
    up_gate_in, up_value_in, gate_taps_in, value_taps_in, down_in, post_ffn_in,
    out,
    wm, wf, xs, xn, val, glu, act, pm, rm, pf, rf, mid, upg, upv, hid, st, gains, taps_b, taps, gtaps_b, vtaps_b,
    ssem, rsem, lsem, psend, precv,
):
    p = Place()
    core = p.core
    partner = p.partner()

    def trade(n, src, dst):
        return pltpu.make_async_remote_copy(
            src_ref=src, dst_ref=dst, send_sem=psend.at[n], recv_sem=precv.at[n], device_id=partner, device_id_type=MESH
        )

    def load(src, dst, n):
        return pltpu.make_async_copy(src, dst, lsem.at[n])

    for i, w in enumerate((value_in, gate_in, proj_in)):
        load(w, wm.at[i, p.zl, p.y, p.x], 0).start()
    for i, w in enumerate((up_gate_in, up_value_in, down_in)):
        load(w, wf.at[i, p.zl, p.y, p.x], 1).start()
    for i, v in enumerate((pre_mix_in, post_mix_in, pre_ffn_in, post_ffn_in, bias_in, chan_in)):
        load(v, gains.at[core, i], 2).start()
    small = [load(stream_in.at[0], xs.at[core], 3), load(taps_in, taps_b, 4), load(gate_taps_in, gtaps_b, 5), load(value_taps_in, vtaps_b, 6)]
    for c in small:
        c.start()
    barrier(p)
    for n, whole in enumerate((wm.at[:, p.zl, p.y, p.x], wf.at[:, p.zl, p.y, p.x])):
        load(whole, whole, n).wait()
    units, base = [], 0
    for u, (ffn, m, lo, cols, split) in enumerate(UNITS):
        units.append(Unit(p, wf if ffn else wm, m, lo, cols, split, ssem, rsem, u, base))
        base += Unit.semaphores(cols, split)
    swap_x = trade(0, xs.at[core], xs.at[core])
    swap_g = trade(1, gains.at[core], gains.at[core])

    def start():
        load(gains.at[core], gains.at[core], 2).wait()
        for c in small:
            c.wait()
        swap_x.start()
        swap_g.start()
        taps[0:31, :] = taps_b[...].astype(F32)
        glu[0:32, :] = jnp.zeros((32, HALF), F32)
        upg[0:8, :] = jnp.zeros((8, HID), F32)
        upv[0:8, :] = jnp.zeros((8, HID), F32)

    def first_norm(i, _):
        r = pl.ds(pl.multiple_of(i * 16, 16), 16)
        a, b = xs[0, r, :].astype(F32), xs[1, r, :].astype(F32)
        inv = norm_rows(a, b, 2 * HALF)
        xn[0, r, :] = (a * inv * gains[0, 0]).astype(BF16)
        xn[1, r, :] = (b * inv * gains[1, 0]).astype(BF16)
        return 0

    def norm():
        trade(0, xs.at[1 - core], xs.at[1 - core]).wait_recv()
        trade(1, gains.at[1 - core], gains.at[1 - core]).wait_recv()
        lax.fori_loop(0, ROWS // 16, first_norm, 0, unroll=2)

    def product(buf, m, c):
        w0 = buf[m, 0, :, :, :, c].reshape(HALF, c.size)
        w1 = buf[m, 1, :, :, :, c].reshape(HALF, c.size)
        return jnp.dot(xn[0], w0, preferred_element_type=F32) + jnp.dot(xn[1], w1, preferred_element_type=F32)

    def blocks(first, width, body):
        def one(i, _):
            body(pl.ds(pl.multiple_of(first + i * 256, 256), 256))
            return 0

        lax.fori_loop(0, width // 256, one, 0)
        if width % 256:
            body(pl.ds(first + width // 256 * 256, width % 256))

    def glu_block(c):
        v, g = product(wm, 0, c), product(wm, 1, c)
        glu[32 : 32 + ROWS, c] = (v * jax.nn.sigmoid(g)).astype(BF16).astype(F32)

    def conv_block(i, _):
        c = pl.ds(pl.multiple_of((i // 8) * 128, 128), 128)
        t = pl.multiple_of((i % 8) * 64, 64)
        g = glu[pl.ds(t, 96), c]
        total = jnp.broadcast_to(gains[core, 4, :, c], (64, 128))
        for k in range(8):
            part = None
            rows = 72 if k else 64
            for j in range(31):
                if (2 + j) % 8 == k:
                    at = (2 + j) // 8 * 8
                    term = taps[j : j + 1, c] * g[at : at + rows]
                    part = term if part is None else part + term
            total = total + part[k : k + 64]
        val[pl.ds(t, 64), c] = total
        return 0

    def stats_block(i, _):
        r = pl.ds(pl.multiple_of(i * 32, 32), 32)
        v = val[r, :]
        mean = jnp.sum(v, axis=1, keepdims=True) * (1.0 / HALF)
        d = v - mean
        st[core, 0, r, :] = jnp.broadcast_to(mean, (32, 128))
        st[core, 1, r, :] = jnp.broadcast_to(jnp.sum(d * d, axis=1, keepdims=True), (32, 128))
        return 0

    def act_block(i, _):
        r = pl.ds(pl.multiple_of(i * 32, 32), 32)
        m0, m1 = st[0, 0, r, :][:, :1], st[1, 0, r, :][:, :1]
        gap = m0 - m1
        var = (st[0, 1, r, :][:, :1] + st[1, 1, r, :][:, :1] + gap * gap * (HALF / 2)) * (0.5 / HALF)
        h = (val[r, :] - (m0 + m1) * 0.5) * lax.rsqrt(var + EPS) * gains[core, 5]
        act[r, :] = jax.nn.silu(h).astype(BF16)
        return 0

    def region(ref, i):
        return ref.at[i // 2, :, pl.ds(512 * (i % 2), 512)]

    def rows_product(lhs, buf, part, total, mine, theirs, base, lo, hi):
        def send(i):
            trade(base, region(mine, i), region(theirs, i)).start()

        for i in range(lo, hi):
            h, n = i // 2, i % 2
            w = buf[2, h, 2 * n : 2 * n + 2, :, :, part].reshape(512, part.size)
            c = pl.ds(512 * n, 512)
            term = lax.dot_general(lhs[:, part], w, (((1,), (1,)), ((), ())), preferred_element_type=F32)
            if mine is None:
                total[h][0:ROWS, c] = term
                continue
            mine[h, :, c] = (term if total is None else total[h][0:ROWS, c] + term).astype(BF16)
            if i > lo:
                send(i - 1)
        if mine is not None:
            send(hi - 1)

    def middle_block(i, _):
        r = pl.ds(pl.multiple_of(i * 16, 16), 16)
        a = (pm[0, r, :].astype(F32) + rm[0, r, :].astype(F32)).astype(BF16).astype(F32)
        b = (pm[1, r, :].astype(F32) + rm[1, r, :].astype(F32)).astype(BF16).astype(F32)
        inv = norm_rows(a, b, 2 * HALF)
        a = (xs[0, r, :].astype(F32) + a * inv * gains[0, 1]).astype(BF16)
        b = (xs[1, r, :].astype(F32) + b * inv * gains[1, 1]).astype(BF16)
        mid[0, r, :] = a
        mid[1, r, :] = b
        a, b = a.astype(F32), b.astype(F32)
        inv = norm_rows(a, b, 2 * HALF)
        xn[0, r, :] = (a * inv * gains[0, 2]).astype(BF16)
        xn[1, r, :] = (b * inv * gains[1, 2]).astype(BF16)
        return 0

    def up_block(c):
        g, v = product(wf, 0, c), product(wf, 1, c)
        upg[8 : 8 + ROWS, c] = g.astype(BF16).astype(F32)
        upv[8 : 8 + ROWS, c] = v.astype(BF16).astype(F32)

    def hidden_block(i, _):
        c = pl.ds(pl.multiple_of((i // 8) * 128, 128), 128)
        t = pl.multiple_of((i % 8) * 64, 64)
        g, v = upg[pl.ds(t, 72), c], upv[pl.ds(t, 72), c]
        kg, kv = gtaps_b[:, c].astype(F32), vtaps_b[:, c].astype(F32)
        gc = kg[0:1] * g[6:70] + kg[1:2] * g[7:71] + kg[2:3] * g[8:72]
        vc = kv[0:1] * v[6:70] + kv[1:2] * v[7:71] + kv[2:3] * v[8:72]
        hid[pl.ds(t, 64), c] = (jax.nn.silu(gc) * vc).astype(BF16)
        return 0

    swap_s = trade(2, st.at[core], st.at[core])

    def stats():
        lax.fori_loop(0, ROWS // 32, stats_block, 0, unroll=2)
        swap_s.start()

    def activate():
        trade(2, st.at[1 - core], st.at[1 - core]).wait_recv()
        lax.fori_loop(0, ROWS // 32, act_block, 0, unroll=2)

    def project(i):
        rows_product(act, wm, pl.ds(0, HALF), None, pm, rm, 3, 2 * i, 2 * i + 2)

    def middle(i):
        if i == 0:
            trade(3, rm, rm).wait_recv()
        n = ROWS // 32
        lax.fori_loop(n * i, n * i + n, middle_block, 0, unroll=2)

    def glu_piece(i):
        glu_block(pl.ds(256 * i, 256))

    def conv(i):
        lax.fori_loop(16 * i, 16 * i + 16, conv_block, 0)

    def up(i):
        up_block(pl.ds(256 * i, min(256, HID - 256 * i)))

    def hidden(i):
        lo, hi = ((0, 24), (24, 48), (48, 68), (68, 88))[i]
        lax.fori_loop(lo, hi, hidden_block, 0)

    def down(i):
        part = pl.ds(DOWN[i], DOWN[i + 1] - DOWN[i])
        last = i + 2 == len(DOWN)
        rows_product(hid, wf, part, (val, glu) if i < 1 < len(DOWN) - 1 or i else None, pf if last else None, rf, 4, 0, 4)

    pieces = dict(
        start=start, norm=norm, glu=glu_piece, conv=conv, stats=stats, act=activate, proj=project, mid=middle, up=up, hid=hidden, down=down
    )
    for name, *numbers in SCHEDULE:
        if name == "u":
            u, kind, k = numbers
            for g in range(2):
                units[u].stage(kind, k, g)
        else:
            pieces[name](*numbers)
    trade(4, rf, rf).wait_recv()

    def out_block(i, _):
        r = pl.ds(pl.multiple_of(i * 16, 16), 16)
        a = (pf[core, r, :].astype(F32) + rf[core, r, :].astype(F32)).astype(BF16).astype(F32)
        b = (pf[1 - core, r, :].astype(F32) + rf[1 - core, r, :].astype(F32)).astype(BF16).astype(F32)
        inv = norm_rows(a, b, 2 * HALF)
        out[0, r, :] = (mid[core, r, :].astype(F32) + a * inv * gains[core, 3]).astype(BF16)
        return 0

    lax.fori_loop(0, ROWS // 16, out_block, 0, unroll=4)
    swap_x.wait_send()
    swap_g.wait_send()
    swap_s.wait_send()
    trade(3, pm, pm).wait_send()
    trade(4, pf, pf).wait_send()
    for u in units:
        u.drain()


def per_device(*args):
    arrays = [a.reshape(1, -1) if a.ndim == 1 else a for a in args]
    sems = pltpu.SemaphoreType.DMA
    return pl.pallas_call(
        kernel,
        out_shape=pltpu.VMEM((1, ROWS, HALF), BF16),
        in_specs=[pl.BlockSpec(memory_space=pl.ANY)] * len(arrays),
        out_specs=pl.BlockSpec(memory_space=pltpu.VMEM),
        scratch_shapes=[
            pltpu.VMEM((3, 2, 4, 4, 64, HALF), BF16),
            pltpu.VMEM((3, 2, 4, 4, 64, HID), BF16),
            pltpu.VMEM((2, ROWS, HALF), BF16),
            pltpu.VMEM((2, ROWS, HALF), BF16),
            pltpu.VMEM((ROWS, HALF), F32),
            pltpu.VMEM((32 + ROWS, HALF), F32),
            pltpu.VMEM((ROWS, HALF), BF16),
            pltpu.VMEM((2, ROWS, HALF), BF16),
            pltpu.VMEM((2, ROWS, HALF), BF16),
            pltpu.VMEM((2, ROWS, HALF), BF16),
            pltpu.VMEM((2, ROWS, HALF), BF16),
            pltpu.VMEM((2, ROWS, HALF), BF16),
            pltpu.VMEM((8 + ROWS, HID), F32),
            pltpu.VMEM((8 + ROWS, HID), F32),
            pltpu.VMEM((ROWS, HID), BF16),
            pltpu.VMEM((2, 2, ROWS, 128), F32),
            pltpu.VMEM((2, 6, 1, HALF), F32),
            pltpu.VMEM((31, HALF), BF16),
            pltpu.VMEM((32, HALF), F32),
            pltpu.VMEM((3, HID), BF16),
            pltpu.VMEM((3, HID), BF16),
            sems((len(UNITS),)),
            sems((sum(Unit.semaphores(cols, split) for _, _, _, cols, split in UNITS),)),
            sems((7,)),
            sems((5,)),
            sems((5,)),
        ],
        compiler_params=pltpu.CompilerParams(collective_id=0, has_side_effects=True, vmem_limit_bytes=60 << 20),
    )(*arrays)


def solution(mesh):
    rows = P(("rep", "fs"), None, "tp")
    vector, matrix, taps = P("tp"), P("fs", "tp"), P(None, "tp")
    placed = (
        rows, vector, matrix, matrix, taps, vector, vector, matrix, vector, vector,
        matrix, matrix, taps, taps, matrix, vector,
    )
    return jax.shard_map(per_device, mesh=mesh, in_specs=placed, out_specs=rows, check_vma=False)
```

```python
import functools

import jax
import jax.numpy as jnp
from jax import lax
from jax.experimental import pallas as pl
from jax.experimental.pallas import tpu as pltpu
from jax.sharding import PartitionSpec as P

EPS = 1e-06
MESH = pl.DeviceIdType.MESH
F32, BF16 = jnp.float32, jnp.bfloat16

class Place:
    def __init__(s):
        fs = lax.axis_index("fs"); zh = lax.axis_index("rep")
        s.core = lax.axis_index("tp")
        s.x = fs % 4; s.y = (fs // 4) % 4; s.zl = fs // 16
        s.z = zh * 2 + s.zl
    def dev(s, dx=0, dy=0, dz=0):
        x = (s.x + dx + 4) % 4; y = (s.y + dy + 4) % 4; z = (s.z + dz + 4) % 4
        return (z // 2, (z % 2) * 16 + y * 4 + x, s.core)
    def pair(s, core):
        return (lax.axis_index("rep"), (1 - s.zl) * 16 + s.y * 4 + s.x, core)

    def partner(s):
        return (lax.axis_index("rep"), lax.axis_index("fs"), 1 - s.core)

class Unit:
    WAITS = (6, 7)

    def __init__(s, place, buf, m, lo, cols, split, ssem, rsem, u, base, turns, away):
        s.turns, s.away = turns, away
        s.p, s.buf, s.m = place, buf, m
        s.c1, s.c2, s.all_columns = pl.ds(lo, split), pl.ds(lo + split, cols - split), pl.ds(lo, cols)
        s.ssem, s.rsem = ssem.at[u], rsem
        s.base = (base, base + (13 if split else 0))

    @staticmethod
    def semaphores(cols, split):
        return (13 if split else 0) + (14 if split < cols else 0)

    def region(s, g, kind, part, content, da, db):
        rows = pl.ds(32 * g + 16 * max(part, 0), 32 if part < 0 else 16)
        cols = s.c1 if kind == 1 else s.c2
        z = slice(None) if content is None else content
        first, second = (s.p.x, s.p.y) if g == 0 else (s.p.y, s.p.x)
        a = slice(None) if da is None else (first + da + 4) % 4
        b = (second + db + 4) % 4
        y, x = (b, a) if g == 0 else (a, b)
        return s.buf.at[s.m, z, y, x, rows, cols]

    def copy(s, n, region, dev):
        return pltpu.make_async_remote_copy(
            src_ref=region, dst_ref=region, send_sem=s.ssem, recv_sem=s.rsem.at[n], device_id=dev, device_id_type=MESH
        )

    def drain(s):
        whole = s.buf.reshape(3, 32, *s.buf.shape[4:]).at[s.m, pl.ds(0, 31), :, s.all_columns]
        s.copy(0, whole, s.p.dev()).wait_send()

    def stage(s, kind, k, g):
        if (s.c1 if kind == 1 else s.c2).size == 0:
            return
        mine, other, R = s.p.zl, 1 - s.p.zl, functools.partial(s.region, g, kind)
        sem = s.base[kind - 1] + g * s.WAITS[kind - 1]
        up = s.turns[g] * (1 - 2 * s.p.zl)
        signs = ((0, 1), (1, -1))

        def send(n, region, da=0, db=0, dz=0):
            s.copy(sem + n, region, s.p.dev(da, db, dz) if g == 0 else s.p.dev(db, da, dz)).start()

        def to_z(region):
            s.copy(s.base[0] + 12, region, s.p.dev(0, 0, up)).start()

        def wait(n, region):
            s.copy(sem + n, region, s.p.dev()).wait_recv()

        if (kind, k) == (1, 0):
            for i, d in signs:
                send(i, R(-1, mine, 0, 0), d)
        elif (kind, k) == (1, 1):
            for i, d in signs:
                wait(i, R(-1, mine, -d, 0))
                send(2, R(i, mine, -d, 0), d)
        elif (kind, k) == (1, 2):
            wait(2, R(-1, mine, 2, 0))
            for i, d in signs:
                send(3 + i, R(-1, mine, None, 0), 0, d)
            to_z(R(-1, mine, None, 0))
        elif (kind, k) == (1, 3):
            for i, d in signs:
                wait(3 + i, R(-1, mine, None, -d))
                send(5, R(i, mine, None, -d), 0, d)
                to_z(R(-1, mine, None, -d))
        elif (kind, k) == (1, 4):
            wait(5, R(-1, mine, None, 2))
            to_z(R(-1, mine, None, 2))
        elif (kind, k) == (1, 5):
            if g == 0:
                wait(12, s.buf.at[s.m, other, :, :, :, s.c1])
        elif (kind, k) == (2, 0):
            own = R(-1, mine, 0, 0)
            source = own if s.away is None else s.away.at[s.m, pl.ds(32 * g, 32)]
            pltpu.make_async_remote_copy(
                src_ref=source, dst_ref=own, send_sem=s.ssem, recv_sem=s.rsem.at[sem], device_id=s.p.dev(0, 0, up), device_id_type=MESH
            ).start()
        elif (kind, k) == (2, 1):
            wait(0, R(-1, other, 0, 0))
            for i, d in signs:
                send(1 + i, R(-1, None, 0, 0), d)
        elif (kind, k) == (2, 2):
            for i, d in signs:
                wait(1 + i, R(-1, None, -d, 0))
                send(3, R(i, None, -d, 0), d)
        elif (kind, k) == (2, 3):
            wait(3, R(-1, None, 2, 0))
            for i, d in signs:
                send(4 + i, R(-1, None, None, 0), 0, d)
        elif (kind, k) == (2, 4):
            for i, d in signs:
                wait(4 + i, R(-1, None, None, -d))
                send(6, R(i, None, None, -d), 0, d)
        elif (kind, k) == (2, 5):
            wait(6, R(-1, None, None, 2))


def barrier(p):
    sem = pltpu.get_barrier_semaphore()
    ds = [p.dev(1), p.dev(-1), p.dev(0, 1), p.dev(0, -1), p.dev(0, 0, 1), p.dev(0, 0, -1), p.partner(), p.pair(1 - p.core)]
    for d in ds:
        pl.semaphore_signal(sem, inc=1, device_id=d, device_id_type=MESH)
    pl.semaphore_wait(sem, len(ds))


QUARTER = 512
UNITS = (
    (0, pl.ds(0, 2), 0, QUARTER, 0, (1, -1)),
    (0, 2, 0, QUARTER, 0, (1, -1)),
    (1, pl.ds(0, 2), 0, 768, 384, (-1, 1)),
    (1, pl.ds(0, 2), 768, 640, 384, (-1, -1)),
    (1, 2, 0, 640, 640, (-1, 1)),
    (1, 2, 640, 768, 128, (1, 1)),
)
DOWN = (0, 640, 1408)
SCHEDULE = (
    ("u", 0, 2, 0), ("start",), ("u", 2, 1, 0), ("u", 3, 1, 0), ("u", 4, 1, 0), ("u", 5, 1, 0), ("u", 0, 2, 1),
    ("u", 1, 2, 0), ("u", 2, 1, 1), ("norm",), ("u", 1, 2, 1), ("u", 2, 2, 0), ("u", 3, 1, 1), ("u", 0, 2, 2),
    ("u", 2, 1, 2), ("u", 0, 2, 3), ("u", 1, 2, 2), ("u", 0, 2, 4), ("u", 1, 2, 3), ("u", 2, 1, 3), ("fwd",),
    ("u", 2, 2, 1), ("u", 3, 1, 2), ("u", 3, 2, 0), ("u", 4, 1, 1), ("u", 0, 2, 5), ("glu", 0), ("glu", 1), ("glu", 2),
    ("glu", 3), ("conv", 0), ("u", 1, 2, 4), ("conv", 1), ("u", 2, 1, 4), ("conv", 2), ("u", 2, 2, 2), ("conv", 3),
    ("stats",), ("u", 3, 2, 1), ("u", 5, 1, 1), ("u", 5, 2, 0), ("u", 4, 1, 2), ("u", 1, 2, 5), ("act",),
    ("u", 2, 1, 5), ("u", 2, 2, 3), ("u", 3, 1, 3), ("proj", 0), ("u", 3, 2, 2), ("u", 5, 1, 2), ("u", 5, 2, 1),
    ("proj", 1), ("red",), ("proj", 2), ("u", 2, 2, 4), ("rz", 0), ("mid", 0), ("u", 3, 1, 4), ("u", 3, 2, 3),
    ("u", 4, 1, 3), ("u", 5, 1, 3), ("u", 5, 2, 2), ("rz", 1), ("mid", 1), ("u", 2, 2, 5), ("rz", 2), ("mid", 2),
    ("u", 3, 1, 5), ("u", 3, 2, 4), ("u", 4, 1, 4), ("rz", 3), ("u", 5, 1, 4), ("u", 5, 2, 3), ("mid", 3), ("up", 0),
    ("up", 1), ("u", 3, 2, 5), ("up", 2), ("hid", 0), ("hid", 1), ("up", 3), ("up", 4), ("u", 5, 2, 4), ("up", 5),
    ("hid", 2), ("hid", 3), ("u", 4, 1, 5), ("down", 0), ("u", 5, 1, 5), ("u", 5, 2, 5), ("down", 1),
)
ROWS = 512
HALF = 1024
HID = 1408


def norm_rows(a, b, width):
    total = jnp.sum(a * a, axis=1, keepdims=True) + jnp.sum(b * b, axis=1, keepdims=True)
    return lax.rsqrt(total * (1.0 / width) + EPS)


def kernel(
    stream_in, pre_mix_in, value_in, gate_in, taps_in, bias_in, chan_in, proj_in, post_mix_in, pre_ffn_in,
    up_gate_in, up_value_in, gate_taps_in, value_taps_in, down_in, post_ffn_in,
    out,
    wm, wf, away, xs, xn, xq, val, glu, act, pm, rm, pq, rq, rz, pf, rf, mid, upg, upv, hid, st, mi, gains, taps_b, taps, gtaps_b, vtaps_b, acc,
    ssem, rsem, lsem, psend, precv,
):
    p = Place()
    core = p.core
    partner = p.partner()

    def trade(n, src, dst, device=None):
        return pltpu.make_async_remote_copy(
            src_ref=src, dst_ref=dst, send_sem=psend.at[n], recv_sem=precv.at[n], device_id=device or partner, device_id_type=MESH
        )

    mine = pl.ds(pl.multiple_of(QUARTER * p.zl, QUARTER), QUARTER)
    theirs = pl.ds(pl.multiple_of(QUARTER * (1 - p.zl), QUARTER), QUARTER)
    twin = p.pair(core)

    def load(src, dst, n):
        return pltpu.make_async_copy(src, dst, lsem.at[n])

    for i, w in enumerate((value_in, gate_in, proj_in)):
        load(w.at[:, mine], wm.at[i, p.zl, p.y, p.x], 0).start()
        load(w.at[:, theirs], away.at[i], 7).start()
    for i, w in enumerate((up_gate_in, up_value_in, down_in)):
        load(w, wf.at[i, p.zl, p.y, p.x], 1).start()
    for i, v in enumerate((pre_mix_in, post_mix_in, pre_ffn_in, post_ffn_in, bias_in, chan_in)):
        load(v, gains.at[core, i], 2).start()
    small = [load(stream_in.at[0], xs.at[core], 3), load(taps_in.at[:, mine], taps_b, 4), load(gate_taps_in, gtaps_b, 5), load(value_taps_in, vtaps_b, 6)]
    for c in small:
        c.start()
    barrier(p)
    for n, whole in ((0, wm.at[:, p.zl, p.y, p.x]), (1, wf.at[:, p.zl, p.y, p.x]), (7, away)):
        load(whole, whole, n).wait()
    units, base = [], 0
    for u, (ffn, m, lo, cols, split, turns) in enumerate(UNITS):
        units.append(Unit(p, wf if ffn else wm, m, lo, cols, split, ssem, rsem, u, base, turns, None if ffn else away))
        base += Unit.semaphores(cols, split)
    swap_x = trade(0, xs.at[core], xs.at[core])
    swap_g = trade(1, gains.at[core], gains.at[core])

    def start():
        load(gains.at[core], gains.at[core], 2).wait()
        for c in small:
            c.wait()
        swap_x.start()
        swap_g.start()
        taps[0:31, :] = taps_b[...].astype(F32)
        glu[:, 0:32, :] = jnp.zeros((2, 32, QUARTER), F32)
        upg[0:8, :] = jnp.zeros((8, HID), F32)
        upv[0:8, :] = jnp.zeros((8, HID), F32)

    def first_norm(i, _):
        r = pl.ds(pl.multiple_of(i * 16, 16), 16)
        a, b = xs[0, r, :].astype(F32), xs[1, r, :].astype(F32)
        inv = norm_rows(a, b, 2 * HALF)
        xn[0, r, :] = (a * inv * gains[0, 0]).astype(BF16)
        xn[1, r, :] = (b * inv * gains[1, 0]).astype(BF16)
        return 0

    def norm():
        trade(0, xs.at[1 - core], xs.at[1 - core]).wait_recv()
        trade(1, gains.at[1 - core], gains.at[1 - core]).wait_recv()
        lax.fori_loop(0, ROWS // 16, first_norm, 0, unroll=2)
        trade(5, xn.at[core], xq.at[core], twin).start()

    def forward():
        trade(5, xq.at[core], xq.at[core], twin).wait_recv()
        trade(6, xq.at[core], xq.at[core]).start()

    def product(lhs, buf, m, c):
        w0 = buf[m, 0, :, :, :, c].reshape(HALF, c.size)
        w1 = buf[m, 1, :, :, :, c].reshape(HALF, c.size)
        return jnp.dot(lhs[0], w0, preferred_element_type=F32) + jnp.dot(lhs[1], w1, preferred_element_type=F32)

    def glu_piece(i):
        if i == 2:
            trade(6, xq.at[1 - core], xq.at[1 - core]).wait_recv()
        c = pl.ds(256 * (i % 2), 256)
        lhs = xq if i // 2 else xn
        v, g = product(lhs, wm, 0, c), product(lhs, wm, 1, c)
        glu[i // 2, 32 : 32 + ROWS, c] = (v * jax.nn.sigmoid(g)).astype(BF16).astype(F32)

    def conv(piece):
        def conv_block(i, _):
            first = 256 * (piece % 2) + 128 * (i // 8)
            c = pl.ds(pl.multiple_of(first, 128), 128)
            t = pl.multiple_of((i % 8) * 64, 64)
            g = glu[piece // 2, pl.ds(t, 96), c]
            bias = gains[core, 4, :, pl.ds(pl.multiple_of(QUARTER * p.zl + first, 128), 128)]
            total = jnp.broadcast_to(bias, (64, 128))
            for k in range(8):
                part = None
                rows = 72 if k else 64
                for j in range(31):
                    if (2 + j) % 8 == k:
                        at = (2 + j) // 8 * 8
                        term = taps[j : j + 1, c] * g[at : at + rows]
                        part = term if part is None else part + term
                total = total + part[k : k + 64]
            val[piece // 2, pl.ds(t, 64), c] = total
            return 0

        lax.fori_loop(0, 16, conv_block, 0)

    lane = lax.broadcasted_iota(jnp.int32, (32, 128), 1)
    owner = (p.zl, 1 - p.zl)
    slot = 2 * p.zl + core
    stats_to = ((2, partner, 2 * p.zl + 1 - core), (7, twin, 2 * (1 - p.zl) + core), (8, p.pair(1 - core), 2 * (1 - p.zl) + 1 - core))

    def stats():
        def block(i, tiles):
            r = pl.ds(pl.multiple_of(i * 32, 32), 32)
            means, squares = tiles
            for q in range(2):
                v = val[q, r, :]
                mean = jnp.sum(v, axis=1, keepdims=True) * (1.0 / QUARTER)
                d = v - mean
                here = lane == 16 * owner[q] + i
                means = jnp.where(here, mean, means)
                squares = jnp.where(here, jnp.sum(d * d, axis=1, keepdims=True), squares)
            return means, squares

        zero = jnp.zeros((32, 128), F32)
        st[slot, 0], st[slot, 1] = lax.fori_loop(0, ROWS // 32, block, (zero, zero), unroll=2)
        for n, device, _ in stats_to:
            trade(n, st.at[slot], st.at[slot], device).start()

    def activate():
        for n, device, source in stats_to:
            trade(n, st.at[source], st.at[source], device).wait_recv()
        mean = (st[0, 0] + st[1, 0] + st[2, 0] + st[3, 0]) * 0.25
        square = jnp.zeros((32, 128), F32)
        for k in range(4):
            d = st[k, 0] - mean
            square = square + (st[k, 1] + d * d * QUARTER)
        mi[0] = mean
        mi[1] = lax.rsqrt(square * (0.5 / HALF) + EPS)
        gain = gains[core, 5, :, mine]

        def block(i, _):
            r = pl.ds(pl.multiple_of(i * 32, 32), 32)
            for q in range(2):
                here = lane == 16 * owner[q] + i
                m = jnp.sum(jnp.where(here, mi[0], 0.0), axis=1, keepdims=True)
                inv = jnp.sum(jnp.where(here, mi[1], 0.0), axis=1, keepdims=True)
                act[q, r, :] = jax.nn.silu((val[q, r, :] - m) * inv * gain).astype(BF16)
            return 0

        lax.fori_loop(0, ROWS // 32, block, 0, unroll=2)

    def region(ref, i):
        return ref.at[i // 2, :, pl.ds(512 * (i % 2), 512)]

    def rows_product(lhs, buf, part, total, mine, theirs, base, lo, hi):
        def send(i):
            trade(base, region(mine, i), region(theirs, i)).start()

        for i in range(lo, hi):
            h, n = i // 2, i % 2
            w = buf[2, h, 2 * n : 2 * n + 2, :, :, part].reshape(512, part.size)
            c = pl.ds(512 * n, 512)
            term = lax.dot_general(lhs[:, part], w, (((1,), (1,)), ((), ())), preferred_element_type=F32)
            if mine is None:
                total[h, :, c] = term
                continue
            mine[h, :, c] = (term if total is None else total[h, :, c] + term).astype(BF16)
            if i > lo and theirs is not None:
                send(i - 1)
        if mine is not None and theirs is not None:
            send(hi - 1)

    def middle_block(i, _):
        r = pl.ds(pl.multiple_of(i * 16, 16), 16)
        a = (pm[0, r, :].astype(F32) + rm[0, r, :].astype(F32) + rz[0, r, :].astype(F32)).astype(BF16).astype(F32)
        b = (pm[1, r, :].astype(F32) + rm[1, r, :].astype(F32) + rz[1, r, :].astype(F32)).astype(BF16).astype(F32)
        inv = norm_rows(a, b, 2 * HALF)
        a = (xs[0, r, :].astype(F32) + a * inv * gains[0, 1]).astype(BF16)
        b = (xs[1, r, :].astype(F32) + b * inv * gains[1, 1]).astype(BF16)
        mid[0, r, :] = a
        mid[1, r, :] = b
        a, b = a.astype(F32), b.astype(F32)
        inv = norm_rows(a, b, 2 * HALF)
        xn[0, r, :] = (a * inv * gains[0, 2]).astype(BF16)
        xn[1, r, :] = (b * inv * gains[1, 2]).astype(BF16)
        return 0

    def up_block(c):
        g, v = product(xn, wf, 0, c), product(xn, wf, 1, c)
        upg[8 : 8 + ROWS, c] = g.astype(BF16).astype(F32)
        upv[8 : 8 + ROWS, c] = v.astype(BF16).astype(F32)

    def hidden_block(i, _):
        c = pl.ds(pl.multiple_of((i // 8) * 128, 128), 128)
        t = pl.multiple_of((i % 8) * 64, 64)
        g, v = upg[pl.ds(t, 72), c], upv[pl.ds(t, 72), c]
        kg, kv = gtaps_b[:, c].astype(F32), vtaps_b[:, c].astype(F32)
        gc = kg[0:1] * g[6:70] + kg[1:2] * g[7:71] + kg[2:3] * g[8:72]
        vc = kv[0:1] * v[6:70] + kv[1:2] * v[7:71] + kv[2:3] * v[8:72]
        hid[pl.ds(t, 64), c] = (jax.nn.silu(gc) * vc).astype(BF16)
        return 0

    def project(i):
        part = pl.ds(0, QUARTER)
        if i:
            rows_product(act.at[0], wm, part, None, pm, rm, 3, 2 * i - 2, 2 * i)
            return
        rows_product(act.at[1], wm, part, None, pq, None, None, 0, 4)
        trade(17, pq.at[1 - core], rq).start()

    def chunk(k):
        return pl.ds(128 * k, 128)

    def reduce():
        trade(17, rq, rq).wait_recv()
        for k in range(4):

            def block(i, _):
                r = pl.ds(pl.multiple_of(i * 32, 32), 32)
                pq[core, r, :] = (pq[core, r, :].astype(F32) + rq[r, :].astype(F32)).astype(BF16)
                return 0

            lax.fori_loop(4 * k, 4 * k + 4, block, 0, unroll=2)
            trade(9 + k, pq.at[core, chunk(k)], rz.at[core, chunk(k)], twin).start()

    def relay(k):
        here = rz.at[core, chunk(k)]
        trade(9 + k, here, here, twin).wait_recv()
        trade(13 + k, here, here).start()

    def middle(k):
        if k == 0:
            trade(3, rm, rm).wait_recv()
            trade(5, xn.at[core], xq.at[core], twin).wait_send()
        there = rz.at[1 - core, chunk(k)]
        trade(13 + k, there, there).wait_recv()
        lax.fori_loop(8 * k, 8 * k + 8, middle_block, 0, unroll=2)

    def up(i):
        up_block(pl.ds(256 * i, min(256, HID - 256 * i)))

    def hidden(i):
        lo, hi = ((0, 24), (24, 48), (48, 68), (68, 88))[i]
        lax.fori_loop(lo, hi, hidden_block, 0)

    def down(i):
        part = pl.ds(DOWN[i], DOWN[i + 1] - DOWN[i])
        last = i + 2 == len(DOWN)
        rows_product(hid, wf, part, acc if i < 1 < len(DOWN) - 1 or i else None, pf if last else None, rf, 4, 0, 4)

    pieces = dict(
        start=start, norm=norm, glu=glu_piece, conv=conv, stats=stats, act=activate, proj=project, red=reduce, rz=relay, fwd=forward, mid=middle, up=up, hid=hidden, down=down
    )
    for name, *numbers in SCHEDULE:
        if name == "u":
            u, kind, k = numbers
            for g in range(2):
                units[u].stage(kind, k, g)
        else:
            pieces[name](*numbers)
    trade(4, rf, rf).wait_recv()

    def out_block(i, _):
        r = pl.ds(pl.multiple_of(i * 16, 16), 16)
        a = (pf[core, r, :].astype(F32) + rf[core, r, :].astype(F32)).astype(BF16).astype(F32)
        b = (pf[1 - core, r, :].astype(F32) + rf[1 - core, r, :].astype(F32)).astype(BF16).astype(F32)
        inv = norm_rows(a, b, 2 * HALF)
        out[0, r, :] = (mid[core, r, :].astype(F32) + a * inv * gains[core, 3]).astype(BF16)
        return 0

    lax.fori_loop(0, ROWS // 16, out_block, 0, unroll=4)
    swap_x.wait_send()
    swap_g.wait_send()
    for n, device, _ in stats_to:
        trade(n, st.at[slot], st.at[slot], device).wait_send()
    trade(6, xq.at[core], xq.at[core]).wait_send()
    trade(17, pq.at[1 - core], rq).wait_send()
    for k in range(4):
        trade(9 + k, pq.at[core, chunk(k)], rz.at[core, chunk(k)], twin).wait_send()
        trade(13 + k, rz.at[core, chunk(k)], rz.at[core, chunk(k)]).wait_send()
    trade(3, pm, pm).wait_send()
    trade(4, pf, pf).wait_send()
    for u in units:
        u.drain()


def per_device(*args):
    arrays = [a.reshape(1, -1) if a.ndim == 1 else a for a in args]
    sems = pltpu.SemaphoreType.DMA
    return pl.pallas_call(
        kernel,
        out_shape=pltpu.VMEM((1, ROWS, HALF), BF16),
        in_specs=[pl.BlockSpec(memory_space=pl.ANY)] * len(arrays),
        out_specs=pl.BlockSpec(memory_space=pltpu.VMEM),
        scratch_shapes=[
            pltpu.VMEM((3, 2, 4, 4, 64, QUARTER), BF16),
            pltpu.VMEM((3, 2, 4, 4, 64, HID), BF16),
            pltpu.VMEM((3, 64, QUARTER), BF16),
            pltpu.VMEM((2, ROWS, HALF), BF16),
            pltpu.VMEM((2, ROWS, HALF), BF16),
            pltpu.VMEM((2, ROWS, HALF), BF16),
            pltpu.VMEM((2, ROWS, QUARTER), F32),
            pltpu.VMEM((2, 32 + ROWS, QUARTER), F32),
            pltpu.VMEM((2, ROWS, QUARTER), BF16),
            pltpu.VMEM((2, ROWS, HALF), BF16),
            pltpu.VMEM((2, ROWS, HALF), BF16),
            pltpu.VMEM((2, ROWS, HALF), BF16),
            pltpu.VMEM((ROWS, HALF), BF16),
            pltpu.VMEM((2, ROWS, HALF), BF16),
            pltpu.VMEM((2, ROWS, HALF), BF16),
            pltpu.VMEM((2, ROWS, HALF), BF16),
            pltpu.VMEM((2, ROWS, HALF), BF16),
            pltpu.VMEM((8 + ROWS, HID), F32),
            pltpu.VMEM((8 + ROWS, HID), F32),
            pltpu.VMEM((ROWS, HID), BF16),
            pltpu.VMEM((4, 2, 32, 128), F32),
            pltpu.VMEM((2, 32, 128), F32),
            pltpu.VMEM((2, 6, 1, HALF), F32),
            pltpu.VMEM((31, QUARTER), BF16),
            pltpu.VMEM((32, QUARTER), F32),
            pltpu.VMEM((3, HID), BF16),
            pltpu.VMEM((3, HID), BF16),
            pltpu.VMEM((2, ROWS, HALF), F32),
            sems((len(UNITS),)),
            sems((sum(Unit.semaphores(cols, split) for _, _, _, cols, split, _ in UNITS),)),
            sems((8,)),
            sems((18,)),
            sems((18,)),
        ],
        compiler_params=pltpu.CompilerParams(collective_id=0, has_side_effects=True, vmem_limit_bytes=62 << 20),
    )(*arrays)


def solution(mesh):
    rows = P(("rep", "fs"), None, "tp")
    vector, matrix, taps = P("tp"), P("fs", "tp"), P(None, "tp")
    placed = (
        rows, vector, matrix, matrix, taps, vector, vector, matrix, vector, vector,
        matrix, matrix, taps, taps, matrix, vector,
    )
    return jax.shard_map(per_device, mesh=mesh, in_specs=placed, out_specs=rows, check_vma=False)
```

```python
import functools

import jax
import jax.numpy as jnp
from jax import lax
from jax.experimental import pallas as pl
from jax.experimental.pallas import tpu as pltpu
from jax.sharding import PartitionSpec as P

EPS = 1e-06
MESH = pl.DeviceIdType.MESH
F32, BF16 = jnp.float32, jnp.bfloat16

class Place:
    def __init__(s):
        fs = lax.axis_index("fs"); zh = lax.axis_index("rep")
        s.core = lax.axis_index("tp")
        s.x = fs % 4; s.y = (fs // 4) % 4; s.zl = fs // 16
        s.z = zh * 2 + s.zl
    def dev(s, dx=0, dy=0, dz=0):
        x = (s.x + dx + 4) % 4; y = (s.y + dy + 4) % 4; z = (s.z + dz + 4) % 4
        return (z // 2, (z % 2) * 16 + y * 4 + x, s.core)
    def pair(s, core):
        return (lax.axis_index("rep"), (1 - s.zl) * 16 + s.y * 4 + s.x, core)

    def partner(s):
        return (lax.axis_index("rep"), lax.axis_index("fs"), 1 - s.core)

class Unit:
    WAITS = (6, 7)

    def __init__(s, place, buf, m, lo, cols, split, ssem, rsem, u, base, turns, away):
        s.turns, s.away = turns, away
        s.p, s.buf, s.m = place, buf, m
        s.c1, s.c2, s.all_columns = pl.ds(lo, split), pl.ds(lo + split, cols - split), pl.ds(lo, cols)
        s.ssem, s.rsem = ssem.at[u], rsem
        s.base = (base, base + (13 if split else 0))

    @staticmethod
    def semaphores(cols, split):
        return (13 if split else 0) + (14 if split < cols else 0)

    def region(s, g, kind, part, content, da, db):
        rows = pl.ds(32 * g + 16 * max(part, 0), 32 if part < 0 else 16)
        cols = s.c1 if kind == 1 else s.c2
        z = slice(None) if content is None else content
        first, second = (s.p.x, s.p.y) if g == 0 else (s.p.y, s.p.x)
        a = slice(None) if da is None else (first + da + 4) % 4
        b = (second + db + 4) % 4
        y, x = (b, a) if g == 0 else (a, b)
        return s.buf.at[s.m, z, y, x, rows, cols]

    def copy(s, n, region, dev):
        return pltpu.make_async_remote_copy(
            src_ref=region, dst_ref=region, send_sem=s.ssem, recv_sem=s.rsem.at[n], device_id=dev, device_id_type=MESH
        )

    def drain(s):
        whole = s.buf.reshape(3, 32, *s.buf.shape[4:]).at[s.m, pl.ds(0, 31), :, s.all_columns]
        s.copy(0, whole, s.p.dev()).wait_send()

    def stage(s, kind, k, g):
        if (s.c1 if kind == 1 else s.c2).size == 0:
            return
        mine, other, R = s.p.zl, 1 - s.p.zl, functools.partial(s.region, g, kind)
        sem = s.base[kind - 1] + g * s.WAITS[kind - 1]
        up = s.turns[g] * (1 - 2 * s.p.zl)
        signs = ((0, 1), (1, -1))

        def send(n, region, da=0, db=0, dz=0):
            s.copy(sem + n, region, s.p.dev(da, db, dz) if g == 0 else s.p.dev(db, da, dz)).start()

        def to_z(region):
            s.copy(s.base[0] + 12, region, s.p.dev(0, 0, up)).start()

        def wait(n, region):
            s.copy(sem + n, region, s.p.dev()).wait_recv()

        if (kind, k) == (1, 0):
            for i, d in signs:
                send(i, R(-1, mine, 0, 0), d)
        elif (kind, k) == (1, 1):
            for i, d in signs:
                wait(i, R(-1, mine, -d, 0))
                send(2, R(i, mine, -d, 0), d)
        elif (kind, k) == (1, 2):
            wait(2, R(-1, mine, 2, 0))
            for i, d in signs:
                send(3 + i, R(-1, mine, None, 0), 0, d)
            to_z(R(-1, mine, None, 0))
        elif (kind, k) == (1, 3):
            for i, d in signs:
                wait(3 + i, R(-1, mine, None, -d))
                send(5, R(i, mine, None, -d), 0, d)
                to_z(R(-1, mine, None, -d))
        elif (kind, k) == (1, 4):
            wait(5, R(-1, mine, None, 2))
            to_z(R(-1, mine, None, 2))
        elif (kind, k) == (1, 5):
            if g == 0:
                wait(12, s.buf.at[s.m, other, :, :, :, s.c1])
        elif (kind, k) == (2, 0):
            own = R(-1, mine, 0, 0)
            source = own if s.away is None else s.away.at[s.m, pl.ds(32 * g, 32)]
            pltpu.make_async_remote_copy(
                src_ref=source, dst_ref=own, send_sem=s.ssem, recv_sem=s.rsem.at[sem], device_id=s.p.dev(0, 0, up), device_id_type=MESH
            ).start()
        elif (kind, k) == (2, 1):
            wait(0, R(-1, other, 0, 0))
            for i, d in signs:
                send(1 + i, R(-1, None, 0, 0), d)
        elif (kind, k) == (2, 2):
            for i, d in signs:
                wait(1 + i, R(-1, None, -d, 0))
                send(3, R(i, None, -d, 0), d)
        elif (kind, k) == (2, 3):
            wait(3, R(-1, None, 2, 0))
            for i, d in signs:
                send(4 + i, R(-1, None, None, 0), 0, d)
        elif (kind, k) == (2, 4):
            for i, d in signs:
                wait(4 + i, R(-1, None, None, -d))
                send(6, R(i, None, None, -d), 0, d)
        elif (kind, k) == (2, 5):
            wait(6, R(-1, None, None, 2))


def barrier(p):
    sem = pltpu.get_barrier_semaphore()
    ds = [p.dev(1), p.dev(-1), p.dev(0, 1), p.dev(0, -1), p.dev(0, 0, 1), p.dev(0, 0, -1), p.partner(), p.pair(1 - p.core)]
    for d in ds:
        pl.semaphore_signal(sem, inc=1, device_id=d, device_id_type=MESH)
    pl.semaphore_wait(sem, len(ds))


QUARTER = 512
UNITS = (
    (0, pl.ds(0, 2), 0, QUARTER, 0, (1, -1)),
    (0, 2, 0, QUARTER, 0, (1, -1)),
    (1, pl.ds(0, 2), 0, 768, 384, (-1, 1)),
    (1, pl.ds(0, 2), 768, 640, 384, (-1, -1)),
    (1, 2, 0, 640, 640, (-1, 1)),
    (1, 2, 640, 768, 128, (1, 1)),
)
DOWN = (0, 640, 1408)
SCHEDULE = (
    ("u", 0, 2, 0), ("start",), ("u", 4, 1, 0), ("u", 3, 1, 0), ("u", 5, 1, 0), ("u", 1, 2, 0), ("u", 2, 1, 0),
    ("u", 3, 2, 0), ("u", 0, 2, 1), ("u", 2, 1, 1), ("u", 1, 2, 1), ("u", 2, 2, 0), ("u", 5, 2, 0), ("u", 3, 1, 1),
    ("norm",), ("u", 0, 2, 2), ("u", 2, 1, 2), ("u", 1, 2, 2), ("u", 0, 2, 3), ("u", 2, 1, 3), ("u", 0, 2, 4), ("fwd",),
    ("u", 5, 1, 1), ("u", 1, 2, 3), ("u", 3, 2, 1), ("u", 3, 1, 2), ("u", 2, 2, 1), ("u", 2, 1, 4), ("u", 4, 1, 1),
    ("u", 0, 2, 5), ("glu", 0), ("glu", 1), ("glu", 2), ("conv", 1), ("conv", 0), ("u", 1, 2, 4), ("conv", 2),
    ("u", 5, 1, 2), ("glu", 3), ("conv", 3), ("stats",), ("u", 3, 1, 3), ("u", 2, 2, 2), ("u", 1, 2, 5), ("u", 4, 1, 2),
    ("act",), ("proj", 0), ("u", 2, 2, 3), ("u", 5, 2, 1), ("u", 3, 2, 2), ("proj", 1), ("u", 3, 1, 4), ("red",),
    ("u", 2, 2, 4), ("rz", 0), ("proj", 2), ("mid", 0), ("u", 3, 2, 3), ("u", 2, 2, 5), ("rz", 1), ("u", 4, 1, 3),
    ("rz", 2), ("u", 5, 2, 2), ("u", 3, 2, 4), ("u", 2, 1, 5), ("mid", 1), ("mid", 2), ("u", 4, 1, 4), ("rz", 3),
    ("u", 5, 2, 3), ("u", 3, 1, 5), ("u", 5, 1, 3), ("mid", 3), ("up", 0), ("u", 3, 2, 5), ("up", 1), ("up", 2),
    ("up", 3), ("up", 4), ("hid", 1), ("u", 5, 2, 4), ("up", 5), ("u", 5, 1, 4), ("u", 4, 1, 5), ("hid", 2), ("hid", 3),
    ("hid", 0), ("down", 0), ("u", 5, 1, 5), ("u", 5, 2, 5), ("down", 1),
)
ROWS = 512
HALF = 1024
HID = 1408


def norm_rows(a, b, width):
    total = jnp.sum(a * a, axis=1, keepdims=True) + jnp.sum(b * b, axis=1, keepdims=True)
    return lax.rsqrt(total * (1.0 / width) + EPS)


def kernel(
    stream_in, pre_mix_in, value_in, gate_in, taps_in, bias_in, chan_in, proj_in, post_mix_in, pre_ffn_in,
    up_gate_in, up_value_in, gate_taps_in, value_taps_in, down_in, post_ffn_in,
    out,
    wm, wf, away, xs, xn, xq, val, glu, act, pm, rm, pq, rq, rz, pf, rf, mid, upg, upv, hid, st, mi, gains, taps_b, taps, gtaps_b, vtaps_b, acc,
    ssem, rsem, lsem, psend, precv,
):
    p = Place()
    core = p.core
    partner = p.partner()

    def trade(n, src, dst, device=None):
        return pltpu.make_async_remote_copy(
            src_ref=src, dst_ref=dst, send_sem=psend.at[n], recv_sem=precv.at[n], device_id=device or partner, device_id_type=MESH
        )

    mine = pl.ds(pl.multiple_of(QUARTER * p.zl, QUARTER), QUARTER)
    theirs = pl.ds(pl.multiple_of(QUARTER * (1 - p.zl), QUARTER), QUARTER)
    twin = p.pair(core)

    def load(src, dst, n):
        return pltpu.make_async_copy(src, dst, lsem.at[n])

    for i, w in enumerate((value_in, gate_in, proj_in)):
        load(w.at[:, mine], wm.at[i, p.zl, p.y, p.x], 0).start()
        load(w.at[:, theirs], away.at[i], 7).start()
    for i, w in enumerate((up_gate_in, up_value_in, down_in)):
        load(w, wf.at[i, p.zl, p.y, p.x], 1).start()
    for i, v in enumerate((pre_mix_in, post_mix_in, pre_ffn_in, post_ffn_in, bias_in, chan_in)):
        load(v, gains.at[core, i], 2).start()
    small = [load(stream_in.at[0], xs.at[core], 3), load(taps_in.at[:, mine], taps_b, 4), load(gate_taps_in, gtaps_b, 5), load(value_taps_in, vtaps_b, 6)]
    for c in small:
        c.start()
    barrier(p)
    for n, whole in ((0, wm.at[:, p.zl, p.y, p.x]), (1, wf.at[:, p.zl, p.y, p.x]), (7, away)):
        load(whole, whole, n).wait()
    units, base = [], 0
    for u, (ffn, m, lo, cols, split, turns) in enumerate(UNITS):
        units.append(Unit(p, wf if ffn else wm, m, lo, cols, split, ssem, rsem, u, base, turns, None if ffn else away))
        base += Unit.semaphores(cols, split)
    swap_x = trade(0, xs.at[core], xs.at[core])
    swap_g = trade(1, gains.at[core], gains.at[core])

    def start():
        load(gains.at[core], gains.at[core], 2).wait()
        for c in small:
            c.wait()
        swap_x.start()
        swap_g.start()
        taps[0:31, :] = taps_b[...].astype(F32)
        glu[:, 0:32, :] = jnp.zeros((2, 32, QUARTER), F32)
        upg[0:8, :] = jnp.zeros((8, HID), F32)
        upv[0:8, :] = jnp.zeros((8, HID), F32)

    def first_norm(i, _):
        r = pl.ds(pl.multiple_of(i * 16, 16), 16)
        a, b = xs[0, r, :].astype(F32), xs[1, r, :].astype(F32)
        inv = norm_rows(a, b, 2 * HALF)
        xn[0, r, :] = (a * inv * gains[0, 0]).astype(BF16)
        xn[1, r, :] = (b * inv * gains[1, 0]).astype(BF16)
        return 0

    def norm():
        trade(0, xs.at[1 - core], xs.at[1 - core]).wait_recv()
        trade(1, gains.at[1 - core], gains.at[1 - core]).wait_recv()
        lax.fori_loop(0, ROWS // 16, first_norm, 0, unroll=2)
        trade(5, xn.at[core], xq.at[core], twin).start()

    def forward():
        trade(5, xq.at[core], xq.at[core], twin).wait_recv()
        trade(6, xq.at[core], xq.at[core]).start()

    def product(lhs, buf, m, c):
        w0 = buf[m, 0, :, :, :, c].reshape(HALF, c.size)
        w1 = buf[m, 1, :, :, :, c].reshape(HALF, c.size)
        return jnp.dot(lhs[0], w0, preferred_element_type=F32) + jnp.dot(lhs[1], w1, preferred_element_type=F32)

    def glu_piece(i):
        if i == 2:
            trade(6, xq.at[1 - core], xq.at[1 - core]).wait_recv()
        c = pl.ds(256 * (i % 2), 256)
        lhs = xq if i // 2 else xn
        v, g = product(lhs, wm, 0, c), product(lhs, wm, 1, c)
        glu[i // 2, 32 : 32 + ROWS, c] = (v * jax.nn.sigmoid(g)).astype(BF16).astype(F32)

    def conv(piece):
        def conv_block(i, _):
            first = 256 * (piece % 2) + 128 * (i // 8)
            c = pl.ds(pl.multiple_of(first, 128), 128)
            t = pl.multiple_of((i % 8) * 64, 64)
            g = glu[piece // 2, pl.ds(t, 96), c]
            bias = gains[core, 4, :, pl.ds(pl.multiple_of(QUARTER * p.zl + first, 128), 128)]
            total = jnp.broadcast_to(bias, (64, 128))
            for k in range(8):
                part = None
                rows = 72 if k else 64
                for j in range(31):
                    if (2 + j) % 8 == k:
                        at = (2 + j) // 8 * 8
                        term = taps[j : j + 1, c] * g[at : at + rows]
                        part = term if part is None else part + term
                total = total + part[k : k + 64]
            val[piece // 2, pl.ds(t, 64), c] = total
            return 0

        lax.fori_loop(0, 16, conv_block, 0)

    lane = lax.broadcasted_iota(jnp.int32, (32, 128), 1)
    owner = (p.zl, 1 - p.zl)
    slot = 2 * p.zl + core
    stats_to = ((2, partner, 2 * p.zl + 1 - core), (7, twin, 2 * (1 - p.zl) + core), (8, p.pair(1 - core), 2 * (1 - p.zl) + 1 - core))

    def stats():
        def block(i, tiles):
            r = pl.ds(pl.multiple_of(i * 32, 32), 32)
            means, squares = tiles
            for q in range(2):
                v = val[q, r, :]
                mean = jnp.sum(v, axis=1, keepdims=True) * (1.0 / QUARTER)
                d = v - mean
                here = lane == 16 * owner[q] + i
                means = jnp.where(here, mean, means)
                squares = jnp.where(here, jnp.sum(d * d, axis=1, keepdims=True), squares)
            return means, squares

        zero = jnp.zeros((32, 128), F32)
        st[slot, 0], st[slot, 1] = lax.fori_loop(0, ROWS // 32, block, (zero, zero), unroll=2)
        for n, device, _ in stats_to:
            trade(n, st.at[slot], st.at[slot], device).start()

    def activate():
        for n, device, source in stats_to:
            trade(n, st.at[source], st.at[source], device).wait_recv()
        mean = (st[0, 0] + st[1, 0] + st[2, 0] + st[3, 0]) * 0.25
        square = jnp.zeros((32, 128), F32)
        for k in range(4):
            d = st[k, 0] - mean
            square = square + (st[k, 1] + d * d * QUARTER)
        mi[0] = mean
        mi[1] = lax.rsqrt(square * (0.5 / HALF) + EPS)
        gain = gains[core, 5, :, mine]

        def block(i, _):
            r = pl.ds(pl.multiple_of(i * 32, 32), 32)
            for q in range(2):
                here = lane == 16 * owner[q] + i
                m = jnp.sum(jnp.where(here, mi[0], 0.0), axis=1, keepdims=True)
                inv = jnp.sum(jnp.where(here, mi[1], 0.0), axis=1, keepdims=True)
                act[q, r, :] = jax.nn.silu((val[q, r, :] - m) * inv * gain).astype(BF16)
            return 0

        lax.fori_loop(0, ROWS // 32, block, 0, unroll=2)

    def region(ref, i):
        return ref.at[i // 2, :, pl.ds(512 * (i % 2), 512)]

    def rows_product(lhs, buf, part, total, mine, theirs, base, lo, hi):
        def send(i):
            trade(base, region(mine, i), region(theirs, i)).start()

        for i in range(lo, hi):
            h, n = i // 2, i % 2
            w = buf[2, h, 2 * n : 2 * n + 2, :, :, part].reshape(512, part.size)
            c = pl.ds(512 * n, 512)
            term = lax.dot_general(lhs[:, part], w, (((1,), (1,)), ((), ())), preferred_element_type=F32)
            if mine is None:
                total[h, :, c] = term
                continue
            mine[h, :, c] = (term if total is None else total[h, :, c] + term).astype(BF16)
            if i > lo and theirs is not None:
                send(i - 1)
        if mine is not None and theirs is not None:
            send(hi - 1)

    def middle_block(i, _):
        r = pl.ds(pl.multiple_of(i * 16, 16), 16)
        a = (pm[0, r, :].astype(F32) + rm[0, r, :].astype(F32) + rz[0, r, :].astype(F32)).astype(BF16).astype(F32)
        b = (pm[1, r, :].astype(F32) + rm[1, r, :].astype(F32) + rz[1, r, :].astype(F32)).astype(BF16).astype(F32)
        inv = norm_rows(a, b, 2 * HALF)
        a = (xs[0, r, :].astype(F32) + a * inv * gains[0, 1]).astype(BF16)
        b = (xs[1, r, :].astype(F32) + b * inv * gains[1, 1]).astype(BF16)
        mid[0, r, :] = a
        mid[1, r, :] = b
        a, b = a.astype(F32), b.astype(F32)
        inv = norm_rows(a, b, 2 * HALF)
        xn[0, r, :] = (a * inv * gains[0, 2]).astype(BF16)
        xn[1, r, :] = (b * inv * gains[1, 2]).astype(BF16)
        return 0

    def up_block(c):
        g, v = product(xn, wf, 0, c), product(xn, wf, 1, c)
        upg[8 : 8 + ROWS, c] = g.astype(BF16).astype(F32)
        upv[8 : 8 + ROWS, c] = v.astype(BF16).astype(F32)

    def hidden_block(i, _):
        c = pl.ds(pl.multiple_of((i // 8) * 128, 128), 128)
        t = pl.multiple_of((i % 8) * 64, 64)
        g, v = upg[pl.ds(t, 72), c], upv[pl.ds(t, 72), c]
        kg, kv = gtaps_b[:, c].astype(F32), vtaps_b[:, c].astype(F32)
        gc = kg[0:1] * g[6:70] + kg[1:2] * g[7:71] + kg[2:3] * g[8:72]
        vc = kv[0:1] * v[6:70] + kv[1:2] * v[7:71] + kv[2:3] * v[8:72]
        hid[pl.ds(t, 64), c] = (jax.nn.silu(gc) * vc).astype(BF16)
        return 0

    def project(i):
        part = pl.ds(0, QUARTER)
        if i:
            rows_product(act.at[0], wm, part, None, pm, rm, 3, 2 * i - 2, 2 * i)
            return
        rows_product(act.at[1], wm, part, None, pq, None, None, 0, 4)
        trade(17, pq.at[1 - core], rq).start()

    def chunk(k):
        return pl.ds(128 * k, 128)

    def reduce():
        trade(17, rq, rq).wait_recv()
        for k in range(4):

            def block(i, _):
                r = pl.ds(pl.multiple_of(i * 32, 32), 32)
                pq[core, r, :] = (pq[core, r, :].astype(F32) + rq[r, :].astype(F32)).astype(BF16)
                return 0

            lax.fori_loop(4 * k, 4 * k + 4, block, 0, unroll=2)
            trade(9 + k, pq.at[core, chunk(k)], rz.at[core, chunk(k)], twin).start()

    def relay(k):
        here = rz.at[core, chunk(k)]
        trade(9 + k, here, here, twin).wait_recv()
        trade(13 + k, here, here).start()

    def middle(k):
        if k == 0:
            trade(3, rm, rm).wait_recv()
            trade(5, xn.at[core], xq.at[core], twin).wait_send()
        there = rz.at[1 - core, chunk(k)]
        trade(13 + k, there, there).wait_recv()
        lax.fori_loop(8 * k, 8 * k + 8, middle_block, 0, unroll=2)

    def up(i):
        up_block(pl.ds(256 * i, min(256, HID - 256 * i)))

    def hidden(i):
        lo, hi = ((0, 24), (24, 48), (48, 68), (68, 88))[i]
        lax.fori_loop(lo, hi, hidden_block, 0, unroll=2)

    def down(i):
        part = pl.ds(DOWN[i], DOWN[i + 1] - DOWN[i])
        last = i + 2 == len(DOWN)
        rows_product(hid, wf, part, acc if i < 1 < len(DOWN) - 1 or i else None, pf if last else None, rf, 4, 0, 4)

    pieces = dict(
        start=start, norm=norm, glu=glu_piece, conv=conv, stats=stats, act=activate, proj=project, red=reduce, rz=relay, fwd=forward, mid=middle, up=up, hid=hidden, down=down
    )
    for name, *numbers in SCHEDULE:
        if name == "u":
            u, kind, k = numbers
            for g in range(2):
                units[u].stage(kind, k, g)
        else:
            pieces[name](*numbers)
    trade(4, rf, rf).wait_recv()

    def out_block(i, _):
        r = pl.ds(pl.multiple_of(i * 16, 16), 16)
        a = (pf[core, r, :].astype(F32) + rf[core, r, :].astype(F32)).astype(BF16).astype(F32)
        b = (pf[1 - core, r, :].astype(F32) + rf[1 - core, r, :].astype(F32)).astype(BF16).astype(F32)
        inv = norm_rows(a, b, 2 * HALF)
        out[0, r, :] = (mid[core, r, :].astype(F32) + a * inv * gains[core, 3]).astype(BF16)
        return 0

    lax.fori_loop(0, ROWS // 16, out_block, 0, unroll=4)
    swap_x.wait_send()
    swap_g.wait_send()
    for n, device, _ in stats_to:
        trade(n, st.at[slot], st.at[slot], device).wait_send()
    trade(6, xq.at[core], xq.at[core]).wait_send()
    trade(17, pq.at[1 - core], rq).wait_send()
    for k in range(4):
        trade(9 + k, pq.at[core, chunk(k)], rz.at[core, chunk(k)], twin).wait_send()
        trade(13 + k, rz.at[core, chunk(k)], rz.at[core, chunk(k)]).wait_send()
    trade(3, pm, pm).wait_send()
    trade(4, pf, pf).wait_send()
    for u in units:
        u.drain()


def per_device(*args):
    arrays = [a.reshape(1, -1) if a.ndim == 1 else a for a in args]
    sems = pltpu.SemaphoreType.DMA
    return pl.pallas_call(
        kernel,
        out_shape=pltpu.VMEM((1, ROWS, HALF), BF16),
        in_specs=[pl.BlockSpec(memory_space=pl.ANY)] * len(arrays),
        out_specs=pl.BlockSpec(memory_space=pltpu.VMEM),
        scratch_shapes=[
            pltpu.VMEM((3, 2, 4, 4, 64, QUARTER), BF16),
            pltpu.VMEM((3, 2, 4, 4, 64, HID), BF16),
            pltpu.VMEM((3, 64, QUARTER), BF16),
            pltpu.VMEM((2, ROWS, HALF), BF16),
            pltpu.VMEM((2, ROWS, HALF), BF16),
            pltpu.VMEM((2, ROWS, HALF), BF16),
            pltpu.VMEM((2, ROWS, QUARTER), F32),
            pltpu.VMEM((2, 32 + ROWS, QUARTER), F32),
            pltpu.VMEM((2, ROWS, QUARTER), BF16),
            pltpu.VMEM((2, ROWS, HALF), BF16),
            pltpu.VMEM((2, ROWS, HALF), BF16),
            pltpu.VMEM((2, ROWS, HALF), BF16),
            pltpu.VMEM((ROWS, HALF), BF16),
            pltpu.VMEM((2, ROWS, HALF), BF16),
            pltpu.VMEM((2, ROWS, HALF), BF16),
            pltpu.VMEM((2, ROWS, HALF), BF16),
            pltpu.VMEM((2, ROWS, HALF), BF16),
            pltpu.VMEM((8 + ROWS, HID), F32),
            pltpu.VMEM((8 + ROWS, HID), F32),
            pltpu.VMEM((ROWS, HID), BF16),
            pltpu.VMEM((4, 2, 32, 128), F32),
            pltpu.VMEM((2, 32, 128), F32),
            pltpu.VMEM((2, 6, 1, HALF), F32),
            pltpu.VMEM((31, QUARTER), BF16),
            pltpu.VMEM((32, QUARTER), F32),
            pltpu.VMEM((3, HID), BF16),
            pltpu.VMEM((3, HID), BF16),
            pltpu.VMEM((2, ROWS, HALF), F32),
            sems((len(UNITS),)),
            sems((sum(Unit.semaphores(cols, split) for _, _, _, cols, split, _ in UNITS),)),
            sems((8,)),
            sems((18,)),
            sems((18,)),
        ],
        compiler_params=pltpu.CompilerParams(collective_id=0, has_side_effects=True, vmem_limit_bytes=62 << 20),
    )(*arrays)


def solution(mesh):
    rows = P(("rep", "fs"), None, "tp")
    vector, matrix, taps = P("tp"), P("fs", "tp"), P(None, "tp")
    placed = (
        rows, vector, matrix, matrix, taps, vector, vector, matrix, vector, vector,
        matrix, matrix, taps, taps, matrix, vector,
    )
    return jax.shard_map(per_device, mesh=mesh, in_specs=placed, out_specs=rows, check_vma=False)
```
